32 devices in a mesh: sp: 4 (over y, x), tp: 8 (over z, core).
Axes of the slice: x: 2, y: 2, z: 4, core: 2. Of those that a mesh axis runs over, the one named last changes fastest.
Arguments:
- tokens: bfloat16 [8, 512, 4096], P('tp', 'sp'), may hold values from -6 to 6
- latent_down_matrix: bfloat16 [4096, 512], P('tp'), may hold values from -0.09375 to 0.09375
- rope_weight: bfloat16 [4096, 64], P('tp'), may hold values from -0.09375 to 0.09375
- latent_norm_scale: float32 [512], replicated, may hold values from 0.1 to 1.9
- key_up_matrix: bfloat16 [512, 32, 128], P(None, 'tp'), may hold values from -0.25 to 0.25
- value_up_matrix: bfloat16 [512, 32, 128], P(None, 'tp'), may hold values from -0.25 to 0.25
- query: bfloat16 [8, 32, 192], P('sp', 'tp'), may hold values from -126 to 126
Outputs:
- plain_key_cache: bfloat16 [8, 512, 32, 128], P('sp', None, 'tp')
- head_value_cache: bfloat16 [8, 512, 32, 128], P('sp', None, 'tp')
- rotated_key_cache: bfloat16 [8, 512, 64], P('sp')
- first_read: bfloat16 [8, 32, 128], P('sp', 'tp')
The draws below stay inside these ranges and needn't reach their ends.
All inputs are finite; a program needn't handle non-finite values.
Results may differ from the reference program's by a relative error of at most 0.035.
Values may be sent and summed in bfloat16 or wider, within the bound.
A program may use at most 64 MiB of HBM per device.

```python
import jax
import jax.numpy as jnp
from jax import lax

MODEL_WIDTH = 4096
LATENT_WIDTH = 512
ROPE = 64
PLAIN_KEY_WIDTH = 128
VALUE_WIDTH = 128
ATTENTION_HEADS = 32
SEQUENCE_COUNT = 8
SEQUENCE_LENGTH = 512


def draw_query(key, part):
    base = jnp.clip(jax.random.normal(jax.random.fold_in(key, 11), (SEQUENCE_COUNT, ATTENTION_HEADS, PLAIN_KEY_WIDTH + ROPE), jnp.float32), -3.5, 3.5) * 3.0
    return base.astype(jnp.bfloat16)


def block_scale(key, dims, split, least, top_value):
    level = 1.0
    for dim, parts in split:
        heights = jax.random.uniform(jax.random.fold_in(jax.random.fold_in(key, 6), dim), (parts,), jnp.float32, least / len(split), top_value / len(split))
        level = level * jnp.repeat(jnp.exp(heights), dims[dim] // parts).reshape((-1,) + (1,) * (len(dims) - 1 - dim))
    return level


def gaussian(rng, shape, scale, most, cuts=(), kind=jnp.bfloat16):
    factor_of = block_scale(rng, shape, cuts, -0.22, 0.18) if cuts else 1.0
    array = jax.random.normal(rng, shape, jnp.float32) * scale * factor_of
    return jnp.minimum(jnp.maximum(array, -most), most).astype(kind)


def setup_inputs(seed: int = 0) -> dict:
    key_list = jax.random.split(jax.random.key(seed), 8)
    return {
        "tokens": gaussian(key_list[0], (SEQUENCE_COUNT, SEQUENCE_LENGTH, MODEL_WIDTH), 1.0, 6.0, ((0, 8), (1, 4))),
        "latent_down_matrix": gaussian(key_list[1], (MODEL_WIDTH, LATENT_WIDTH), MODEL_WIDTH ** -0.5, 0.09375, ((0, 8),)),
        "rope_weight": gaussian(key_list[2], (MODEL_WIDTH, ROPE), MODEL_WIDTH ** -0.5, 0.09375, ((0, 8),)),
        "latent_norm_scale": jnp.clip(1.0 + 0.18 * jax.random.normal(key_list[3], (LATENT_WIDTH,), jnp.float32), 0.1, 1.9),
        "key_up_matrix": gaussian(key_list[4], (LATENT_WIDTH, ATTENTION_HEADS, PLAIN_KEY_WIDTH), LATENT_WIDTH ** -0.5, 0.25, ((1, 8),)),
        "value_up_matrix": gaussian(key_list[5], (LATENT_WIDTH, ATTENTION_HEADS, VALUE_WIDTH), LATENT_WIDTH ** -0.5, 0.25, ((1, 8),)),
        "query": draw_query(jax.random.fold_in(key_list[7], 71), 0),
    }


def rotate(part, positions):
    half = part.shape[-1] // 2
    freqs = 1.0 / 10000.0 ** (jnp.arange(half, dtype=jnp.float32) * 2.0 / part.shape[-1])
    angles = positions.astype(jnp.float32)[:, None] * freqs
    cosine = jnp.cos(angles)
    sine = jnp.sin(angles)
    first = part[..., :half]
    second = part[..., half:]
    return jnp.concatenate([first * cosine - second * sine, second * cosine + first * sine], axis=-1)

def reference(tokens, latent_down_matrix, rope_weight, latent_norm_scale, key_up_matrix, value_up_matrix, query):
    flat = tokens.reshape(SEQUENCE_COUNT * SEQUENCE_LENGTH, MODEL_WIDTH)
    latent = jnp.dot(flat, latent_down_matrix, preferred_element_type=jnp.float32)
    scaled = latent * lax.rsqrt(lax.optimization_barrier(jnp.mean(latent * latent, axis=-1, keepdims=True)) + 1e-06)
    latent_normalized = (scaled * latent_norm_scale.astype(jnp.float32)).astype(jnp.bfloat16)
    rope = jnp.dot(flat, rope_weight, preferred_element_type=jnp.float32).reshape(SEQUENCE_COUNT, SEQUENCE_LENGTH, ROPE)
    positions = jnp.arange(SEQUENCE_LENGTH, dtype=jnp.int32)
    rotated_key_cache = rotate(rope, positions).astype(jnp.bfloat16)
    plain_key_cache = jnp.dot(latent_normalized, key_up_matrix.reshape(LATENT_WIDTH, ATTENTION_HEADS * PLAIN_KEY_WIDTH), preferred_element_type=jnp.float32).astype(jnp.bfloat16).reshape(SEQUENCE_COUNT, SEQUENCE_LENGTH, ATTENTION_HEADS, PLAIN_KEY_WIDTH)
    head_value_cache = jnp.dot(latent_normalized, value_up_matrix.reshape(LATENT_WIDTH, ATTENTION_HEADS * VALUE_WIDTH), preferred_element_type=jnp.float32).astype(jnp.bfloat16).reshape(SEQUENCE_COUNT, SEQUENCE_LENGTH, ATTENTION_HEADS, VALUE_WIDTH)
    query_float = query.astype(jnp.float32)
    query_plain = query[..., :PLAIN_KEY_WIDTH]
    rotated_query = rotate(query_float[..., PLAIN_KEY_WIDTH:], jnp.full((1,), SEQUENCE_LENGTH, jnp.int32)).astype(jnp.bfloat16)
    factor = 1.0 / (PLAIN_KEY_WIDTH + ROPE) ** 0.5

    def attend(items):
        plain, turned, keys, values, rotary = items
        scores = jnp.einsum('hd,lhd->hl', plain.astype(jnp.float32), keys.astype(jnp.float32))
        scores = scores + jnp.einsum('hd,ld->hl', turned.astype(jnp.float32), rotary.astype(jnp.float32))
        scores = scores * factor
        weights = jnp.exp(scores - lax.optimization_barrier(jnp.max(scores, axis=-1, keepdims=True)))
        total = lax.optimization_barrier(jnp.sum(weights, axis=-1, keepdims=True))
        rounded = weights.astype(jnp.bfloat16)
        mixed = jnp.einsum('hl,lhd->hd', rounded.astype(jnp.float32), values.astype(jnp.float32))
        return (mixed / total).astype(jnp.bfloat16)
    first_read = lax.map(attend, (query_plain, rotated_query, plain_key_cache, head_value_cache, rotated_key_cache))
    return (plain_key_cache, head_value_cache, rotated_key_cache, first_read)
```

```python
import functools

import numpy as np
import jax
import jax.numpy as jnp
from jax import lax
from jax.sharding import PartitionSpec as P
from jax.experimental import pallas as pl
from jax.experimental.pallas import tpu as pltpu

CORES = 2
BF16 = jnp.bfloat16
F32 = jnp.float32


def turn_tables(positions, width):
    half = width // 2
    freqs = (1.0 / np.float32(10000.0) ** (np.arange(half, dtype=np.float32) * np.float32(2.0) / np.float32(width))).astype(np.float32)
    angles = positions.astype(np.float32)[:, None] * freqs
    cosine = np.cos(angles).astype(np.float32)
    sine = np.sin(angles).astype(np.float32)
    return np.concatenate([cosine, cosine], -1), np.concatenate([-sine, sine], -1)


def turn(part, cosine, sine):
    half = part.shape[-1] // 2
    swapped = jnp.concatenate([part[:, half:], part[:, :half]], axis=-1)
    return part * cosine + swapped * sine


def move_kernel(planes, spots, tok, wl, wr, scale, cos_ref, sin_ref, kup, vup, x_out, up_out,
                tokens, wlat, wrope, acc, other, spread, kbuf, vbuf,
                tok_s, tok_r, own_s, z_s, z_r, x_s, x_r, y_s, y_r, dx_s, dx_r, dy_s, dy_r,
                acc_s, acc_r, g_s, g_r, f_s, f_r, p_s, p_r, up_s):
    s = lax.axis_index("sp")
    t = lax.axis_index("tp")
    z = t // CORES
    c = t % CORES
    rows, lat = wl.shape
    rope = wr.shape[1]
    span = tok.shape[1]
    quarter = rows // 4
    eighth = quarter // 2
    q = s % 4
    base = s - q

    def flip(bit):
        if bit == 1:
            return s + 1 - 2 * (s % 2)
        return s + 2 - 4 * ((s // 2) % 2)

    sx = flip(1)
    sy = flip(2)

    def dev(si, zi, ci):
        return {"sp": si, "tp": zi * CORES + ci}

    def remote(src, dst, ss, rs, where):
        return pltpu.make_async_remote_copy(
            src_ref=src, dst_ref=dst, send_sem=ss, recv_sem=rs,
            device_id=where, device_id_type=pl.DeviceIdType.MESH)

    def own_tok(u):
        cols = pl.ds(pl.multiple_of((u * CORES + c) * rows, 128), rows)
        return pltpu.make_async_copy(tok.at[0, :, cols], tokens.at[0, u], own_s.at[u])

    def part_tok(u):
        cols = pl.ds(pl.multiple_of((u * CORES + 1 - c) * rows, 128), rows)
        return remote(tok.at[0, :, cols], tokens.at[1, u], tok_s.at[u], tok_r.at[u], dev(s, z, 1 - c))

    own_wl = pltpu.make_async_copy(wl, wlat.at[z], own_s.at[planes])
    own_wr = pltpu.make_async_copy(wr, wrope.at[z], own_s.at[planes + 1])
    get_k = pltpu.make_async_copy(kup, kbuf, up_s.at[0])
    get_v = pltpu.make_async_copy(vup, vbuf, up_s.at[1])
    own_wl.start()
    own_wr.start()

    barrier = pltpu.get_barrier_semaphore()

    def greet(where):
        pl.semaphore_signal(barrier, inc=1, device_id=where, device_id_type=pl.DeviceIdType.MESH)

    for i in range(1, planes):
        greet(dev(s, lax.rem(z + i, planes), c))
    for i in range(1, spots):
        greet(dev(lax.rem(s + i, spots), z, c))
    greet(dev(s, z, 1 - c))
    for u in range(planes):
        own_tok(u).start()
    own_wl.wait()
    own_wr.wait()
    pl.semaphore_wait(barrier, planes - 1 + spots - 1 + 1)

    def piece(u, start, count, sems, rsems, where):
        start = pl.multiple_of(start, 16)
        a = remote(wlat.at[u, pl.ds(start, count)], wlat.at[u, pl.ds(start, count)],
                   sems.at[0, u], rsems.at[0, u], where)
        b = remote(wrope.at[u, pl.ds(start, count)], wrope.at[u, pl.ds(start, count)],
                   sems.at[1, u], rsems.at[1, u], where)
        return a, b

    def each(pair, what):
        for p in pair:
            getattr(p, what)()

    qx = q + 1 - 2 * (q % 2)
    qy = q + 2 - 4 * (q // 2)
    qd = 3 - q

    def z_up(u):
        return piece(u, q * quarter, quarter, z_s, z_r, dev(s, z + 1, c))

    def z_down(u):
        a, b = piece(u, q * quarter, quarter, z_s, z_r, dev(s, z - 1, c))
        return a, b

    def z_up_own():
        start = pl.multiple_of(q * quarter, 16)
        return (remote(wlat.at[z, pl.ds(start, quarter)], wlat.at[z, pl.ds(start, quarter)], z_s.at[2, 0], z_r.at[0, z], dev(s, z + 1, c)),
                remote(wrope.at[z, pl.ds(start, quarter)], wrope.at[z, pl.ds(start, quarter)], z_s.at[2, 1], z_r.at[1, z], dev(s, z + 1, c)))

    def x_copy(u):
        return piece(u, q * quarter, quarter, x_s, x_r, dev(sx, z, c))

    def y_copy(u):
        return piece(u, q * quarter, quarter, y_s, y_r, dev(sy, z, c))

    def x_in(u):
        return piece(u, qx * quarter, quarter, x_s, x_r, dev(sx, z, c))

    def y_in(u):
        return piece(u, qy * quarter, quarter, y_s, y_r, dev(sy, z, c))

    def dy_copy(u):
        return piece(u, qx * quarter, eighth, dy_s, dy_r, dev(sy, z, c))

    def dx_copy(u):
        return piece(u, qy * quarter + eighth, eighth, dx_s, dx_r, dev(sx, z, c))

    def dy_in(u):
        return piece(u, qd * quarter, eighth, dy_s, dy_r, dev(sy, z, c))

    def dx_in(u):
        return piece(u, qd * quarter + eighth, eighth, dx_s, dx_r, dev(sx, z, c))

    @pl.when(z + 1 < planes)
    def _():
        each(z_up_own(), "start")

    @pl.when(z > 0)
    def _():
        each(z_down(z), "start")

    for u in range(planes):
        part_tok(u).start()
    get_k.start()
    get_v.start()

    def block_dot(u):
        x = tokens[:, u].reshape(CORES * span, rows)
        return (jnp.dot(x, wlat[u], preferred_element_type=F32),
                jnp.dot(x, wrope[u], preferred_element_type=F32))

    def load_tokens(u):
        own_tok(u).wait()
        part_tok(u).wait()

    for u in range(planes):
        load_tokens(u)
    a, b = block_dot(z)
    acc[:, :, :lat] = a.reshape(CORES, span, lat)
    acc[:, :, lat:] = b.reshape(CORES, span, rope)

    def reshape_up():
        get_k.wait()
        get_v.wait()
        heads = kbuf.shape[1]
        kw = kbuf.shape[2]
        vw = vbuf.shape[2]
        k = kbuf[...].astype(F32)
        v = vbuf[...].astype(F32)
        for h in range(heads):
            up_out[:, h * kw:(h + 1) * kw] = k[:, h, :].astype(BF16)
            up_out[:, heads * kw + h * vw:heads * kw + (h + 1) * vw] = v[:, h, :].astype(BF16)

    def step(d, carry):
        for sign in (-1, 1):
            u = z + sign * d

            @pl.when((u >= 0) & (u < planes))
            def _():
                each(piece(u, q * quarter, quarter, z_s, z_r, dev(s, z, 1 - c)), "wait_recv")
                if sign < 0:
                    @pl.when(z + 1 < planes)
                    def _():
                        each(z_up(u), "start")
                else:
                    @pl.when(z > 0)
                    def _():
                        each(z_down(u), "start")
                each(x_copy(u), "start")
                each(y_copy(u), "start")
        for sign in (-1, 1):
            u = z + sign * (d - 1)

            @pl.when((u >= 0) & (u < planes) & (d > 1))
            def _():
                each(x_in(u), "wait_recv")
                each(dy_copy(u), "start")
                each(y_in(u), "wait_recv")
                each(dx_copy(u), "start")
        for sign in (-1, 1):
            u = z + sign * (d - 2)

            @pl.when((u >= 0) & (u < planes) & (d > 2))
            def _():
                each(dy_in(u), "wait_recv")
                each(dx_in(u), "wait_recv")
                a, b = block_dot(u)
                acc[:, :, :lat] += a.reshape(CORES, span, lat)
                acc[:, :, lat:] += b.reshape(CORES, span, rope)
        return carry

    reshape_up()
    lax.fori_loop(1, planes + 2, step, 0)

    swap = remote(acc.at[1], other, acc_s, acc_r, dev(s, z, 1 - c))
    swap.start()
    swap.wait()
    latent = acc[0, :, :lat] + other[:, :lat]
    ropes = acc[0, :, lat:] + other[:, lat:]
    scaled = latent * lax.rsqrt(jnp.mean(latent * latent, axis=-1, keepdims=True) + 1e-06)
    spread[z, :, :lat] = (scaled * scale[...]).astype(BF16)
    spread[z, :, lat:] = turn(ropes, cos_ref[...], sin_ref[...]).astype(BF16)

    def g_copy(u, zi, slot):
        return remote(spread.at[u], spread.at[u], g_s.at[slot, u], g_r.at[u], dev(s, zi, c))

    def f_copy(u):
        return remote(spread.at[u], x_out.at[c, s], f_s.at[u], f_r.at[s], dev(u, z, c))

    def f_in(si):
        return remote(spread.at[0], x_out.at[c, si], f_s.at[0], f_r.at[si], dev(si, z, c))

    def p_copy(si):
        return remote(x_out.at[c, si], x_out.at[c, si], p_s.at[si], p_r.at[si], dev(s, z, 1 - c))

    def p_in(si):
        return remote(x_out.at[1 - c, si], x_out.at[1 - c, si], p_s.at[si], p_r.at[si], dev(s, z, 1 - c))

    own_copy = pltpu.make_async_copy(spread.at[s], x_out.at[c, s], own_s.at[0])

    def g_up(u):
        return g_copy(u, z + 1, 0)

    def g_down(u):
        return g_copy(u, z - 1, 1)

    def deliver(u):
        @pl.when(u != s)
        def _():
            f_copy(u).start()

        @pl.when(u == s)
        def _():
            own_copy.start()

    @pl.when(z + 1 < planes)
    def _():
        g_up(z).start()

    @pl.when(z > 0)
    def _():
        g_down(z).start()

    deliver(z)

    def g_step(d, carry):
        for sign in (-1, 1):
            u = z + sign * d

            @pl.when((u >= 0) & (u < planes))
            def _():
                g_copy(u, z, 0).wait_recv()
                if sign < 0:
                    @pl.when(z + 1 < planes)
                    def _():
                        g_up(u).start()
                else:
                    @pl.when(z > 0)
                    def _():
                        g_down(u).start()
                deliver(u)
        return carry

    lax.fori_loop(1, planes, g_step, 0)
    own_copy.wait()
    p_copy(s).start()

    def p_step(i, carry):
        si = lax.rem(s + i, spots)
        f_in(si).wait_recv()
        p_copy(si).start()
        return carry

    lax.fori_loop(1, spots, p_step, 0)

    def p_drain(si, carry):
        p_in(si).wait_recv()
        p_copy(si).wait_send()
        return carry

    lax.fori_loop(0, spots, p_drain, 0)

    def drain(u, carry):
        @pl.when(u != s)
        def _():
            f_copy(u).wait_send()

        @pl.when((u <= z) & (z + 1 < planes))
        def _():
            g_up(u).wait_send()

        @pl.when((u >= z) & (z > 0))
        def _():
            g_down(u).wait_send()

        @pl.when((u < z) & (z + 1 < planes))
        def _():
            each(z_up(u), "wait_send")

        @pl.when((u >= z) & (z > 0))
        def _():
            each(z_down(u), "wait_send")

        @pl.when(u != z)
        def _():
            each(x_copy(u), "wait_send")
            each(y_copy(u), "wait_send")
            each(dy_copy(u), "wait_send")
            each(dx_copy(u), "wait_send")
        return carry

    lax.fori_loop(0, planes, drain, 0)

    @pl.when(z + 1 < planes)
    def _():
        each(z_up_own(), "wait_send")


def read_kernel(x_ref, up_ref, q_ref, cos_ref, sin_ref, plain_ref, value_ref, rot_ref, read_ref, wide):
    length = x_ref.shape[1]
    heads = q_ref.shape[1]
    lat = up_ref.shape[0]
    rope = x_ref.shape[2] - lat
    kw = q_ref.shape[2] - rope
    vw = up_ref.shape[1] // heads - kw
    rotated = x_ref[0, :, lat:]
    rot_ref[0] = rotated
    normed = x_ref[0, :, :lat]
    keys = jnp.dot(normed, up_ref[:, :heads * kw], preferred_element_type=F32)
    values = jnp.dot(normed, up_ref[:, heads * kw:], preferred_element_type=F32)
    for h in range(heads):
        wide[pl.ds(h, length, stride=heads), :] = keys[:, h * kw:(h + 1) * kw]
    plain_ref[0] = wide[...].astype(BF16)
    for h in range(heads):
        wide[pl.ds(h, length, stride=heads), :] = values[:, h * vw:(h + 1) * vw]
    value_ref[0] = wide[...].astype(BF16)
    keys = keys.astype(BF16)
    values = values.astype(BF16)
    query = q_ref[0].astype(F32)
    turned = turn(query[:, kw:], cos_ref[...], sin_ref[...]).astype(BF16)
    tiled = jnp.concatenate([query[:, :kw]] * heads, axis=1)
    row = lax.broadcasted_iota(jnp.int32, tiled.shape, 0)
    col = lax.broadcasted_iota(jnp.int32, tiled.shape, 1)
    blocked = jnp.where(col // kw == row, tiled, 0.0).astype(BF16)
    contract = (((1,), (1,)), ((), ()))
    scores = lax.dot_general(blocked, keys, contract, preferred_element_type=F32)
    scores = scores + lax.dot_general(turned, rotated, contract, preferred_element_type=F32)
    scores = scores * (1.0 / (kw + rope) ** 0.5)
    weights = jnp.exp(scores - jnp.max(scores, axis=-1, keepdims=True))
    total = jnp.sum(weights, axis=-1, keepdims=True)
    mixed = jnp.dot(weights.astype(BF16), values, preferred_element_type=F32) / total
    for h in range(heads):
        read_ref[0, h:h + 1, :] = mixed[h:h + 1, h * vw:(h + 1) * vw].astype(BF16)


def body(planes, spots, tokens, latent_down, rope_weight, norm_scale, key_up, value_up, query):
    span = tokens.shape[1]
    rows, lat = latent_down.shape
    rope = rope_weight.shape[1]
    heads, kw = key_up.shape[1:]
    vw = value_up.shape[2]
    length = spots * span
    cosine, sine = turn_tables(np.arange(length + 1), rope)
    s = lax.axis_index("sp")
    cos_here = lax.dynamic_slice_in_dim(jnp.asarray(cosine), s * span, span, 0)
    sin_here = lax.dynamic_slice_in_dim(jnp.asarray(sine), s * span, span, 0)
    vmem = pl.BlockSpec(memory_space=pltpu.VMEM)
    hbm = pl.BlockSpec(memory_space=pl.ANY)
    dma = pltpu.SemaphoreType.DMA
    x_all, up = pl.pallas_call(
        functools.partial(move_kernel, planes, spots),
        out_shape=(jax.ShapeDtypeStruct((CORES, spots, span, lat + rope), BF16),
                   jax.ShapeDtypeStruct((lat, heads * (kw + vw)), BF16)),
        in_specs=[hbm, vmem, vmem, vmem, vmem, vmem, hbm, hbm],
        out_specs=(vmem, vmem),
        scratch_shapes=[
            pltpu.VMEM((CORES, planes, span, rows), BF16),
            pltpu.VMEM((planes, rows, lat), BF16),
            pltpu.VMEM((planes, rows, rope), BF16),
            pltpu.VMEM((CORES, span, lat + rope), F32),
            pltpu.VMEM((span, lat + rope), F32),
            pltpu.VMEM((planes, span, lat + rope), BF16),
            pltpu.VMEM(key_up.shape, BF16),
            pltpu.VMEM(value_up.shape, BF16),
            dma((planes,)), dma((planes,)), dma((planes + 2,)),
            dma((3, max(planes, 2))), dma((2, planes)),
            dma((2, planes)), dma((2, planes)), dma((2, planes)), dma((2, planes)),
            dma((2, planes)), dma((2, planes)), dma((2, planes)), dma((2, planes)),
            dma, dma,
            dma((2, planes)), dma((planes,)),
            dma((planes,)), dma((spots,)),
            dma((spots,)), dma((spots,)),
            dma((2,)),
        ],
        compiler_params=pltpu.CompilerParams(collective_id=0, has_side_effects=True),
    )(tokens, latent_down, rope_weight, norm_scale.reshape(1, lat), cos_here, sin_here, key_up, value_up)
    x_all = x_all.reshape(CORES, length, lat + rope)

    def whole(shape):
        return pl.BlockSpec(shape, lambda i: (0,) * len(shape))

    def per(shape):
        return pl.BlockSpec((1,) + shape, lambda i: (i,) + (0,) * len(shape))

    plain, value, rot, read = pl.pallas_call(
        read_kernel,
        grid=(CORES,),
        out_shape=(jax.ShapeDtypeStruct((CORES, length * heads, kw), BF16),
                   jax.ShapeDtypeStruct((CORES, length * heads, vw), BF16),
                   jax.ShapeDtypeStruct((CORES, length, rope), BF16),
                   jax.ShapeDtypeStruct((CORES, heads, vw), BF16)),
        in_specs=[per((length, lat + rope)), whole(up.shape), per(query.shape[1:]), whole((1, rope)), whole((1, rope))],
        out_specs=(per((length * heads, kw)), per((length * heads, vw)), per((length, rope)), per((heads, vw))),
        scratch_shapes=[pltpu.VMEM((length * heads, kw), F32)],
    )(x_all, up, query, jnp.asarray(cosine[length:]), jnp.asarray(sine[length:]))
    return (plain.reshape(CORES, length, heads, kw), value.reshape(CORES, length, heads, vw), rot, read)


def solution(mesh):
    planes = mesh.shape["tp"] // CORES
    spots = mesh.shape["sp"]
    assert planes == spots and spots % 4 == 0
    in_specs = (
        P("tp", "sp", None),
        P("tp", None),
        P("tp", None),
        P(),
        P(None, "tp", None),
        P(None, "tp", None),
        P("sp", "tp", None),
    )
    out_specs = (
        P("sp", None, "tp", None),
        P("sp", None, "tp", None),
        P("sp", None, None),
        P("sp", "tp", None),
    )
    return jax.shard_map(functools.partial(body, planes, spots), mesh=mesh, in_specs=in_specs,
                         out_specs=out_specs, check_vma=False)
```

```python
import functools

import numpy as np
import jax
import jax.numpy as jnp
from jax import lax
from jax.sharding import PartitionSpec as P
from jax.experimental import pallas as pl
from jax.experimental.pallas import tpu as pltpu

CORES = 2
BF16 = jnp.bfloat16
F32 = jnp.float32


def turn_tables(positions, width):
    half = width // 2
    freqs = (1.0 / np.float32(10000.0) ** (np.arange(half, dtype=np.float32) * np.float32(2.0) / np.float32(width))).astype(np.float32)
    angles = positions.astype(np.float32)[:, None] * freqs
    cosine = np.cos(angles).astype(np.float32)
    sine = np.sin(angles).astype(np.float32)
    return np.concatenate([cosine, cosine], -1), np.concatenate([-sine, sine], -1)


def turn(part, cosine, sine):
    half = part.shape[-1] // 2
    swapped = jnp.concatenate([part[:, half:], part[:, :half]], axis=-1)
    return part * cosine + swapped * sine


def move_kernel(planes, spots, tok, wl, wr, scale, cos_hbm, sin_hbm, kup, vup, x_out, rot_out, up_out,
                tokens, wlat, wrope, acc, acct, other, othert, spread, spreadt, kbuf, vbuf, cos_ref, sin_ref,
                tok_s, tok_r, own_s, z_s, z_r, zo_s, x_s, x_r, y_s, y_r, dx_s, dx_r, dy_s, dy_r,
                acc_s, acc_r, g_s, g_r, f_s, f_r, p_s, p_r, up_s):
    s = lax.axis_index("sp")
    t = lax.axis_index("tp")
    z = t // CORES
    c = t % CORES
    rows, lat = wl.shape
    rope = wr.shape[0]
    span = tok.shape[1]
    quarter = rows // 4
    eighth = quarter // 2
    rpart = rope // 4
    half = span // 2
    q = s % 4
    sx = s + 1 - 2 * (s % 2)
    sy = s + 2 - 4 * ((s // 2) % 2)
    qx = q + 1 - 2 * (q % 2)
    qy = q + 2 - 4 * (q // 2)
    qd = 3 - q

    def dev(si, zi, ci):
        return {"sp": si, "tp": zi * CORES + ci}

    here = dev(s, z, 1 - c)

    def remote(src, dst, ss, rs, where):
        return pltpu.make_async_remote_copy(
            src_ref=src, dst_ref=dst, send_sem=ss, recv_sem=rs,
            device_id=where, device_id_type=pl.DeviceIdType.MESH)

    def own_tok(u):
        cols = pl.ds(pl.multiple_of((u * CORES + c) * rows, 128), rows)
        return pltpu.make_async_copy(tok.at[0, :, cols], tokens.at[0, u], own_s.at[u])

    def part_tok(u):
        cols = pl.ds(pl.multiple_of((u * CORES + 1 - c) * rows, 128), rows)
        return remote(tok.at[0, :, cols], tokens.at[1, u], tok_s.at[u], tok_r.at[u], here)

    own_wl = pltpu.make_async_copy(wl, wlat.at[z], own_s.at[planes])
    own_wr = pltpu.make_async_copy(wr, wrope.at[z], own_s.at[planes + 1])
    place = pl.ds(pl.multiple_of(s * span, 128), span)
    get_k = pltpu.make_async_copy(kup, kbuf, up_s.at[0])
    get_v = pltpu.make_async_copy(vup, vbuf, up_s.at[1])
    get_c = pltpu.make_async_copy(cos_hbm.at[:, place], cos_ref, up_s.at[2])
    get_n = pltpu.make_async_copy(sin_hbm.at[:, place], sin_ref, up_s.at[3])
    own_wl.start()
    own_wr.start()

    barrier = pltpu.get_barrier_semaphore()

    def greet(where):
        pl.semaphore_signal(barrier, inc=1, device_id=where, device_id_type=pl.DeviceIdType.MESH)

    for i in range(1, planes):
        greet(dev(s, lax.rem(z + i, planes), c))
    for i in range(1, spots):
        greet(dev(lax.rem(s + i, spots), z, c))
    greet(here)
    for u in range(planes):
        own_tok(u).start()
    own_wl.wait()
    own_wr.wait()
    pl.semaphore_wait(barrier, planes - 1 + spots - 1 + 1)

    def piece(u, part, k, ss, rs, where):
        rng = pl.ds(pl.multiple_of(part * quarter + k * eighth, 16), eighth)
        out = [remote(wlat.at[u, rng], wlat.at[u, rng], ss.at[k, u], rs.at[k, u], where)]
        if k == 0:
            rng = pl.ds(pl.multiple_of(part * rpart, 16), rpart)
            out.append(remote(wrope.at[u, rng], wrope.at[u, rng], ss.at[2, u], rs.at[2, u], where))
        return out

    def each(copies, what):
        for p in copies:
            getattr(p, what)()

    def z_own(k):
        rng = pl.ds(pl.multiple_of(q * quarter + k * eighth, 16), eighth)
        where = dev(s, z + 1, c)
        out = [remote(wlat.at[z, rng], wlat.at[z, rng], zo_s.at[k], z_r.at[k, z], where)]
        if k == 0:
            rng = pl.ds(pl.multiple_of(q * rpart, 16), rpart)
            out.append(remote(wrope.at[z, rng], wrope.at[z, rng], zo_s.at[2], z_r.at[2, z], where))
        return out

    def z_up(u, k):
        return piece(u, q, k, z_s, z_r, dev(s, z + 1, c))

    def z_down(u, k):
        return piece(u, q, k, z_s, z_r, dev(s, z - 1, c))

    def x_copy(u, k):
        return piece(u, q, k, x_s, x_r, dev(sx, z, c))

    def y_copy(u, k):
        return piece(u, q, k, y_s, y_r, dev(sy, z, c))

    def x_in(u, k):
        return piece(u, qx, k, x_s, x_r, here)

    def y_in(u, k):
        return piece(u, qy, k, y_s, y_r, here)

    def dy_copy(u):
        return piece(u, qx, 0, dy_s, dy_r, dev(sy, z, c))

    def dx_copy(u):
        return piece(u, qy, 1, dx_s, dx_r, dev(sx, z, c))

    def dy_in(u):
        return piece(u, qd, 0, dy_s, dy_r, here)

    def dx_in(u):
        return piece(u, qd, 1, dx_s, dx_r, here)

    has_up = z + 1 < planes
    has_down = z > 0
    for k in range(2):
        @pl.when(has_up)
        def _():
            each(z_own(k), "start")

        @pl.when(has_down)
        def _():
            each(z_down(z, k), "start")

    for u in range(planes):
        part_tok(u).start()
    get_k.start()
    get_v.start()
    get_c.start()
    get_n.start()
    contract = (((1,), (1,)), ((), ()))

    def block_dot(u):
        x = tokens[:, u].reshape(CORES * span, rows)
        return (jnp.dot(x, wlat[u], preferred_element_type=F32),
                lax.dot_general(wrope[u], x, contract, preferred_element_type=F32))

    for u in range(planes):
        own_tok(u).wait()
        part_tok(u).wait()
    a, b = block_dot(z)
    acc[...] = a
    acct[...] = b
    get_k.wait()
    get_v.wait()
    get_c.wait()
    get_n.wait()

    def reshape_up():
        heads, kw = kbuf.shape[1:]
        vw = vbuf.shape[2]
        k = kbuf[...].astype(F32)
        v = vbuf[...].astype(F32)
        for h in range(heads):
            up_out[:, h * kw:(h + 1) * kw] = k[:, h, :].astype(BF16)
            up_out[:, heads * kw + h * vw:heads * kw + (h + 1) * vw] = v[:, h, :].astype(BF16)

    def step(d, carry):
        for k in range(2):
            for sign in (-1, 1):
                u = z + sign * d

                @pl.when((u >= 0) & (u < planes))
                def _():
                    each(piece(u, q, k, z_s, z_r, here), "wait_recv")
                    if sign < 0:
                        @pl.when(has_up)
                        def _():
                            each(z_up(u, k), "start")
                    else:
                        @pl.when(has_down)
                        def _():
                            each(z_down(u, k), "start")
                    each(x_copy(u, k), "start")
                    each(y_copy(u, k), "start")

        @pl.when(d == 1)
        def _():
            reshape_up()

        for sign in (-1, 1):
            u = z + sign * (d - 1)

            @pl.when((u >= 0) & (u < planes) & (d > 1))
            def _():
                each(x_in(u, 0), "wait_recv")
                each(dy_copy(u), "start")
                each(y_in(u, 1), "wait_recv")
                each(dx_copy(u), "start")
        for sign in (-1, 1):
            u = z + sign * (d - 2)

            @pl.when((u >= 0) & (u < planes) & (d > 2))
            def _():
                each(x_in(u, 1), "wait_recv")
                each(y_in(u, 0), "wait_recv")
                each(dy_in(u), "wait_recv")
                each(dx_in(u), "wait_recv")
                a, b = block_dot(u)
                acc[...] += a
                acct[...] += b
        return carry

    lax.fori_loop(1, planes + 2, step, 0)

    swaps = [remote(acc.at[pl.ds(span, span)], other, acc_s.at[0], acc_r.at[0], here),
             remote(acct.at[:, pl.ds(span, span)], othert, acc_s.at[1], acc_r.at[1], here)]
    each(swaps, "start")
    each(swaps, "wait")
    latent = acc[:span] + other[...]
    ropes = acct[:, :span] + othert[...]
    scaled = latent * lax.rsqrt(jnp.mean(latent * latent, axis=-1, keepdims=True) + 1e-06)
    spread[z] = (scaled * scale[...]).astype(BF16)
    swapped = jnp.concatenate([ropes[rope // 2:], ropes[:rope // 2]], axis=0)
    spreadt[z] = (ropes * cos_ref[...] + swapped * sin_ref[...]).astype(BF16)

    def g_copy(u, k, zi, slot):
        rng = pl.ds(k * half, half)
        out = [remote(spread.at[u, rng], spread.at[u, rng], g_s.at[slot, k, u], g_r.at[k, u], dev(s, zi, c))]
        if k == 0:
            out.append(remote(spreadt.at[u], spreadt.at[u], g_s.at[slot, 2, u], g_r.at[2, u], dev(s, zi, c)))
        return out

    def lanes(si):
        return pl.ds(pl.multiple_of(si * span, 128), span)

    def f_copy(u, k, where, si):
        rng = pl.ds(k * half, half)
        out = [remote(spread.at[u, rng], x_out.at[c, si, rng], f_s.at[k, u], f_r.at[k, si], where)]
        if k == 0:
            out.append(remote(spreadt.at[u], rot_out.at[c, :, lanes(si)], f_s.at[2, u], f_r.at[2, si], where))
        return out

    def p_copy(ci, si, k):
        rng = pl.ds(k * half, half)
        out = [remote(x_out.at[ci, si, rng], x_out.at[ci, si, rng], p_s.at[k, si], p_r.at[k, si], here)]
        if k == 0:
            part = rot_out.at[ci, :, lanes(si)]
            out.append(remote(part, part, p_s.at[2, si], p_r.at[2, si], here))
        return out

    own_copies = [pltpu.make_async_copy(spread.at[s], x_out.at[c, s], own_s.at[0]),
                  pltpu.make_async_copy(spreadt.at[s], rot_out.at[c, :, lanes(s)], own_s.at[1])]

    def deliver(u, k):
        @pl.when(u != s)
        def _():
            each(f_copy(u, k, dev(u, z, c), s), "start")

        if k == 1:
            @pl.when(u == s)
            def _():
                each(own_copies, "start")

    for k in range(2):
        @pl.when(has_up)
        def _():
            each(g_copy(z, k, z + 1, 0), "start")

        @pl.when(has_down)
        def _():
            each(g_copy(z, k, z - 1, 1), "start")

        deliver(z, k)

    def g_step(d, carry):
        for k in range(2):
            for sign in (-1, 1):
                u = z + sign * d

                @pl.when((u >= 0) & (u < planes))
                def _():
                    each(g_copy(u, k, z, 0), "wait_recv")
                    if sign < 0:
                        @pl.when(has_up)
                        def _():
                            each(g_copy(u, k, z + 1, 0), "start")
                    else:
                        @pl.when(has_down)
                        def _():
                            each(g_copy(u, k, z - 1, 1), "start")
                    deliver(u, k)
        return carry

    lax.fori_loop(1, planes, g_step, 0)
    each(own_copies, "wait")
    for k in range(2):
        each(p_copy(c, s, k), "start")

    def p_step(i, carry):
        si = lax.rem(s + i, spots)
        for k in range(2):
            each(f_copy(0, k, here, si), "wait_recv")
            each(p_copy(c, si, k), "start")
        return carry

    lax.fori_loop(1, spots, p_step, 0)

    def p_drain(si, carry):
        for k in range(2):
            each(p_copy(1 - c, si, k), "wait_recv")
            each(p_copy(c, si, k), "wait_send")
        return carry

    lax.fori_loop(0, spots, p_drain, 0)

    def drain(u, carry):
        for k in range(2):
            @pl.when(u != s)
            def _():
                each(f_copy(u, k, here, s), "wait_send")

            @pl.when((u <= z) & has_up)
            def _():
                each(g_copy(u, k, z, 0), "wait_send")

            @pl.when((u >= z) & has_down)
            def _():
                each(g_copy(u, k, z, 1), "wait_send")
                each(z_down(u, k), "wait_send")

            @pl.when((u < z) & has_up)
            def _():
                each(z_up(u, k), "wait_send")

            @pl.when(u != z)
            def _():
                each(x_copy(u, k), "wait_send")
                each(y_copy(u, k), "wait_send")

        @pl.when(u != z)
        def _():
            each(dy_copy(u), "wait_send")
            each(dx_copy(u), "wait_send")
        return carry

    lax.fori_loop(0, planes, drain, 0)

    @pl.when(has_up)
    def _():
        for k in range(2):
            each(z_own(k), "wait_send")


def read_kernel(x_ref, r_ref, up_ref, q_ref, cos_ref, sin_ref, plain_ref, value_ref, rot_ref, read_ref, wide):
    length = x_ref.shape[1]
    heads = q_ref.shape[1]
    lat = up_ref.shape[0]
    rope = r_ref.shape[1]
    kw = q_ref.shape[2] - rope
    vw = up_ref.shape[1] // heads - kw
    rotated = r_ref[0]
    rot_ref[0] = rotated
    normed = x_ref[0]
    keys = jnp.dot(normed, up_ref[:, :heads * kw], preferred_element_type=F32)
    values = jnp.dot(normed, up_ref[:, heads * kw:], preferred_element_type=F32)
    for h in range(heads):
        wide[pl.ds(h, length, stride=heads), :] = keys[:, h * kw:(h + 1) * kw]
    plain_ref[0] = wide[...].astype(BF16)
    for h in range(heads):
        wide[pl.ds(h, length, stride=heads), :] = values[:, h * vw:(h + 1) * vw]
    value_ref[0] = wide[...].astype(BF16)
    keys = keys.astype(BF16)
    values = values.astype(BF16)
    query = q_ref[0].astype(F32)
    turned = turn(query[:, kw:], cos_ref[...], sin_ref[...]).astype(BF16)
    tiled = jnp.concatenate([query[:, :kw]] * heads, axis=1)
    row = lax.broadcasted_iota(jnp.int32, tiled.shape, 0)
    col = lax.broadcasted_iota(jnp.int32, tiled.shape, 1)
    blocked = jnp.where(col // kw == row, tiled, 0.0).astype(BF16)
    contract = (((1,), (1,)), ((), ()))
    scores = lax.dot_general(blocked, keys, contract, preferred_element_type=F32)
    scores = scores + jnp.dot(turned, rotated, preferred_element_type=F32)
    scores = scores * (1.0 / (kw + rope) ** 0.5)
    weights = jnp.exp(scores - jnp.max(scores, axis=-1, keepdims=True))
    total = jnp.sum(weights, axis=-1, keepdims=True)
    mixed = jnp.dot(weights.astype(BF16), values, preferred_element_type=F32) / total
    for h in range(heads):
        read_ref[0, h:h + 1, :] = mixed[h:h + 1, h * vw:(h + 1) * vw].astype(BF16)


def body(planes, spots, tokens, latent_down, rope_weight, norm_scale, key_up, value_up, query):
    span = tokens.shape[1]
    rows, lat = latent_down.shape
    rope = rope_weight.shape[1]
    heads, kw = key_up.shape[1:]
    vw = value_up.shape[2]
    length = spots * span
    cosine, sine = turn_tables(np.arange(length + 1), rope)
    vmem = pl.BlockSpec(memory_space=pltpu.VMEM)
    hbm = pl.BlockSpec(memory_space=pl.ANY)
    dma = pltpu.SemaphoreType.DMA
    x_all, rot_all, up = pl.pallas_call(
        functools.partial(move_kernel, planes, spots),
        out_shape=(jax.ShapeDtypeStruct((CORES, spots, span, lat), BF16),
                   jax.ShapeDtypeStruct((CORES, rope, length), BF16),
                   jax.ShapeDtypeStruct((lat, heads * (kw + vw)), BF16)),
        in_specs=[hbm, hbm, hbm, vmem, hbm, hbm, hbm, hbm],
        out_specs=(vmem, vmem, vmem),
        scratch_shapes=[
            pltpu.VMEM((CORES, planes, span, rows), BF16),
            pltpu.VMEM((planes, rows, lat), BF16),
            pltpu.VMEM((planes, rope, rows), BF16),
            pltpu.VMEM((CORES * span, lat), F32),
            pltpu.VMEM((rope, CORES * span), F32),
            pltpu.VMEM((span, lat), F32),
            pltpu.VMEM((rope, span), F32),
            pltpu.VMEM((planes, span, lat), BF16),
            pltpu.VMEM((planes, rope, span), BF16),
            pltpu.VMEM(key_up.shape, BF16),
            pltpu.VMEM(value_up.shape, BF16),
            pltpu.VMEM((rope, span), F32),
            pltpu.VMEM((rope, span), F32),
            dma((planes,)), dma((planes,)), dma((planes + 2,)),
            dma((3, planes)), dma((3, planes)), dma((3,)),
            dma((3, planes)), dma((3, planes)), dma((3, planes)), dma((3, planes)),
            dma((3, planes)), dma((3, planes)), dma((3, planes)), dma((3, planes)),
            dma((2,)), dma((2,)),
            dma((2, 3, planes)), dma((3, planes)),
            dma((3, planes)), dma((3, spots)),
            dma((3, spots)), dma((3, spots)),
            dma((4,)),
        ],
        compiler_params=pltpu.CompilerParams(collective_id=0, has_side_effects=True),
    )(tokens, latent_down, rope_weight.T, norm_scale.reshape(1, lat),
      jnp.asarray(np.ascontiguousarray(cosine[:length].T)), jnp.asarray(np.ascontiguousarray(sine[:length].T)),
      key_up, value_up)
    x_all = x_all.reshape(CORES, length, lat)

    def whole(shape):
        return pl.BlockSpec(shape, lambda i: (0,) * len(shape))

    def per(shape):
        return pl.BlockSpec((1,) + shape, lambda i: (i,) + (0,) * len(shape))

    plain, value, rot, read = pl.pallas_call(
        read_kernel,
        grid=(CORES,),
        out_shape=(jax.ShapeDtypeStruct((CORES, length * heads, kw), BF16),
                   jax.ShapeDtypeStruct((CORES, length * heads, vw), BF16),
                   jax.ShapeDtypeStruct((CORES, rope, length), BF16),
                   jax.ShapeDtypeStruct((CORES, heads, vw), BF16)),
        in_specs=[per((length, lat)), per((rope, length)), whole(up.shape), per(query.shape[1:]), whole((1, rope)), whole((1, rope))],
        out_specs=(per((length * heads, kw)), per((length * heads, vw)), per((rope, length)), per((heads, vw))),
        scratch_shapes=[pltpu.VMEM((length * heads, kw), F32)],
    )(x_all, rot_all, up, query, jnp.asarray(cosine[length:]), jnp.asarray(sine[length:]))
    return (plain.reshape(CORES, length, heads, kw), value.reshape(CORES, length, heads, vw), jnp.swapaxes(rot, 1, 2), read)


def solution(mesh):
    planes = mesh.shape["tp"] // CORES
    spots = mesh.shape["sp"]
    assert planes == spots and spots % 4 == 0
    in_specs = (
        P("tp", "sp", None),
        P("tp", None),
        P("tp", None),
        P(),
        P(None, "tp", None),
        P(None, "tp", None),
        P("sp", "tp", None),
    )
    out_specs = (
        P("sp", None, "tp", None),
        P("sp", None, "tp", None),
        P("sp", None, None),
        P("sp", "tp", None),
    )
    return jax.shard_map(functools.partial(body, planes, spots), mesh=mesh, in_specs=in_specs,
                         out_specs=out_specs, check_vma=False)
```

```python
import functools

import numpy as np
import jax
import jax.numpy as jnp
from jax import lax
from jax.sharding import PartitionSpec as P
from jax.experimental import pallas as pl
from jax.experimental.pallas import tpu as pltpu

CORES = 2
PARTS = 4
BF16 = jnp.bfloat16
F32 = jnp.float32


def turn_tables(positions, width):
    half = width // 2
    freqs = (1.0 / np.float32(10000.0) ** (np.arange(half, dtype=np.float32) * np.float32(2.0) / np.float32(width))).astype(np.float32)
    angles = positions.astype(np.float32)[:, None] * freqs
    cosine = np.cos(angles).astype(np.float32)
    sine = np.sin(angles).astype(np.float32)
    return np.concatenate([cosine, cosine], -1), np.concatenate([-sine, sine], -1)


def turn(part, cosine, sine):
    half = part.shape[-1] // 2
    swapped = jnp.concatenate([part[:, half:], part[:, :half]], axis=-1)
    return part * cosine + swapped * sine


def move_kernel(planes, spots, tok, wl, wr, scale, cos_hbm, sin_hbm, kup, vup, x_out, rot_out, up_out,
                tokens, wlat, wrope, acc, acct, other, othert, spread, spreadt, kbuf, vbuf, cos_ref, sin_ref,
                tok_s, tok_r, own_s, z_s, z_r, zo_s, x_s, x_r, y_s, y_r, dx_s, dx_r, dy_s, dy_r,
                acc_s, acc_r, g_s, g_r, f_s, f_r, p_s, p_r, up_s):
    s = lax.axis_index("sp")
    t = lax.axis_index("tp")
    z = t // CORES
    c = t % CORES
    rows, lat = wl.shape
    rope = wr.shape[0]
    span = tok.shape[1]
    quarter = rows // 4
    eighth = quarter // 2
    rpart = rope // 4
    half = span // PARTS
    q = s % 4
    sx = s + 1 - 2 * (s % 2)
    sy = s + 2 - 4 * ((s // 2) % 2)
    qx = q + 1 - 2 * (q % 2)
    qy = q + 2 - 4 * (q // 2)
    qd = 3 - q

    def dev(si, zi, ci):
        return {"sp": si, "tp": zi * CORES + ci}

    here = dev(s, z, 1 - c)

    def remote(src, dst, ss, rs, where):
        return pltpu.make_async_remote_copy(
            src_ref=src, dst_ref=dst, send_sem=ss, recv_sem=rs,
            device_id=where, device_id_type=pl.DeviceIdType.MESH)

    def own_tok(u):
        cols = pl.ds(pl.multiple_of((u * CORES + c) * rows, 128), rows)
        return pltpu.make_async_copy(tok.at[0, :, cols], tokens.at[0, u], own_s.at[u])

    def part_tok(u):
        cols = pl.ds(pl.multiple_of((u * CORES + 1 - c) * rows, 128), rows)
        return remote(tok.at[0, :, cols], tokens.at[1, u], tok_s.at[u], tok_r.at[u], here)

    own_wl = pltpu.make_async_copy(wl, wlat.at[z], own_s.at[planes])
    own_wr = pltpu.make_async_copy(wr, wrope.at[z], own_s.at[planes + 1])
    place = pl.ds(pl.multiple_of(s * span, 128), span)
    get_k = pltpu.make_async_copy(kup, kbuf, up_s.at[0])
    get_v = pltpu.make_async_copy(vup, vbuf, up_s.at[1])
    get_c = pltpu.make_async_copy(cos_hbm.at[:, place], cos_ref, up_s.at[2])
    get_n = pltpu.make_async_copy(sin_hbm.at[:, place], sin_ref, up_s.at[3])
    own_wl.start()
    own_wr.start()

    barrier = pltpu.get_barrier_semaphore()

    def greet(where):
        pl.semaphore_signal(barrier, inc=1, device_id=where, device_id_type=pl.DeviceIdType.MESH)

    for i in range(1, planes):
        greet(dev(s, lax.rem(z + i, planes), c))
    for i in range(1, spots):
        greet(dev(lax.rem(s + i, spots), z, c))
    greet(here)
    for u in range(planes):
        own_tok(u).start()
    own_wl.wait()
    own_wr.wait()
    pl.semaphore_wait(barrier, planes - 1 + spots - 1 + 1)

    def piece(u, part, k, ss, rs, where):
        rng = pl.ds(pl.multiple_of(part * quarter + k * eighth, 16), eighth)
        out = [remote(wlat.at[u, rng], wlat.at[u, rng], ss.at[k, u], rs.at[k, u], where)]
        if k == 0:
            rng = pl.ds(pl.multiple_of(part * rpart, 16), rpart)
            out.append(remote(wrope.at[u, rng], wrope.at[u, rng], ss.at[2, u], rs.at[2, u], where))
        return out

    def each(copies, what):
        for p in copies:
            getattr(p, what)()

    def z_rows(k):
        start = q * quarter + k * eighth if k < 2 else qd * quarter + eighth
        return pl.ds(pl.multiple_of(start, 16), eighth)

    def z_piece(u, k, sems, where):
        rng = z_rows(k)
        i = k if k < 2 else 3
        out = [remote(wlat.at[u, rng], wlat.at[u, rng], sems(i), z_r.at[i, u], where)]
        if k == 0:
            rng = pl.ds(pl.multiple_of(q * rpart, 16), rpart)
            out.append(remote(wrope.at[u, rng], wrope.at[u, rng], sems(2), z_r.at[2, u], where))
        return out

    def z_own(k):
        return z_piece(z, k, lambda i: zo_s.at[i], dev(s, z + 1, c))

    def z_up(u, k):
        return z_piece(u, k, lambda i: z_s.at[i, u], dev(s, z + 1, c))

    def z_down(u, k):
        return z_piece(u, k, lambda i: z_s.at[i, u], dev(s, z - 1, c))

    def z_in(u, k):
        return z_piece(u, k, lambda i: z_s.at[i, u], here)

    def by_y(u):
        return (u + c) % 2 == 0

    def x_copy(u, k):
        return piece(u, q, k, x_s, x_r, dev(sx, z, c))

    def y_copy(u, k):
        return piece(u, q, k, y_s, y_r, dev(sy, z, c))

    def x_in(u, k):
        return piece(u, qx, k, x_s, x_r, here)

    def y_in(u, k):
        return piece(u, qy, k, y_s, y_r, here)

    def dy_copy(u):
        return piece(u, qx, 0, dy_s, dy_r, dev(sy, z, c))

    def dx_copy(u):
        return piece(u, qy, 0, dx_s, dx_r, dev(sx, z, c))

    def dy_in(u):
        return piece(u, qd, 0, dy_s, dy_r, here)

    def dx_in(u):
        return piece(u, qd, 0, dx_s, dx_r, here)

    has_up = z + 1 < planes
    has_down = z > 0
    for k in range(2):
        @pl.when(has_up)
        def _():
            each(z_own(k), "start")

        @pl.when(has_down)
        def _():
            each(z_down(z, k), "start")

    for u in range(planes):
        part_tok(u).start()
    get_k.start()
    get_v.start()
    get_c.start()
    get_n.start()
    contract = (((1,), (1,)), ((), ()))

    def block_dot(u):
        x = tokens[:, u].reshape(CORES * span, rows)
        return (jnp.dot(x, wlat[u], preferred_element_type=F32),
                lax.dot_general(wrope[u], x, contract, preferred_element_type=F32))

    for u in range(planes):
        own_tok(u).wait()
        part_tok(u).wait()
    a, b = block_dot(z)
    acc[...] = a
    acct[...] = b
    get_k.wait()
    get_v.wait()
    get_c.wait()
    get_n.wait()

    def reshape_up():
        heads, kw = kbuf.shape[1:]
        vw = vbuf.shape[2]
        k = kbuf[...].astype(F32)
        v = vbuf[...].astype(F32)
        for h in range(heads):
            up_out[:, h * kw:(h + 1) * kw] = k[:, h, :].astype(BF16)
            up_out[:, heads * kw + h * vw:heads * kw + (h + 1) * vw] = v[:, h, :].astype(BF16)

    def relay(u, k, sign):
        each(z_in(u, k), "wait_recv")
        if sign < 0:
            @pl.when(has_up)
            def _():
                each(z_up(u, k), "start")
        else:
            @pl.when(has_down)
            def _():
                each(z_down(u, k), "start")

    def send_own(k):
        @pl.when(has_up)
        def _():
            each(z_own(k), "start")

        @pl.when(has_down)
        def _():
            each(z_down(z, k), "start")

    def valid(u):
        return (u >= 0) & (u < planes)

    def step(d, carry):
        for k in range(2):
            for sign in (-1, 1):
                u = z + sign * d

                @pl.when(valid(u))
                def _():
                    relay(u, k, sign)
                    each(x_copy(u, k), "start")
                    each(y_copy(u, k), "start")

        @pl.when(d == 1)
        def _():
            reshape_up()

        @pl.when(d == planes - 1)
        def _():
            send_own(2)

        for sign in (-1, 1):
            u = z + sign * (d - 1)

            @pl.when(valid(u) & (d > 1))
            def _():
                @pl.when(by_y(u))
                def _():
                    each(x_in(u, 0), "wait_recv")
                    each(dy_copy(u), "start")

                @pl.when(~by_y(u))
                def _():
                    each(y_in(u, 0), "wait_recv")
                    each(dx_copy(u), "start")
        return carry

    lax.fori_loop(1, planes + 1, step, 0)

    def finish(d, carry):
        for sign in (-1, 1):
            u = z + sign * d

            @pl.when(valid(u))
            def _():
                relay(u, 2, sign)
        for sign in (-1, 1):
            u = z + sign * d

            @pl.when(valid(u))
            def _():
                each(x_in(u, 1), "wait_recv")
                each(y_in(u, 1), "wait_recv")

                @pl.when(by_y(u))
                def _():
                    each(y_in(u, 0), "wait_recv")
                    each(dy_in(u), "wait_recv")

                @pl.when(~by_y(u))
                def _():
                    each(x_in(u, 0), "wait_recv")
                    each(dx_in(u), "wait_recv")
                a, b = block_dot(u)
                acc[...] += a
                acct[...] += b
        return carry

    lax.fori_loop(1, planes, finish, 0)

    swaps = [remote(acc.at[pl.ds(span, span)], other, acc_s.at[0], acc_r.at[0], here),
             remote(acct.at[:, pl.ds(span, span)], othert, acc_s.at[1], acc_r.at[1], here)]
    each(swaps, "start")
    each(swaps, "wait")
    latent = acc[:span] + other[...]
    ropes = acct[:, :span] + othert[...]
    scaled = latent * lax.rsqrt(jnp.mean(latent * latent, axis=-1, keepdims=True) + 1e-06)
    spread[z] = (scaled * scale[...]).astype(BF16)
    swapped = jnp.concatenate([ropes[rope // 2:], ropes[:rope // 2]], axis=0)
    spreadt[z] = (ropes * cos_ref[...] + swapped * sin_ref[...]).astype(BF16)

    def g_copy(u, k, zi, slot):
        rng = pl.ds(k * half, half)
        out = [remote(spread.at[u, rng], spread.at[u, rng], g_s.at[slot, k, u], g_r.at[k, u], dev(s, zi, c))]
        if k == 0:
            out.append(remote(spreadt.at[u], spreadt.at[u], g_s.at[slot, PARTS, u], g_r.at[PARTS, u], dev(s, zi, c)))
        return out

    def lanes(si):
        return pl.ds(pl.multiple_of(si * span, 128), span)

    def f_copy(u, k, where, si):
        rng = pl.ds(k * half, half)
        out = [remote(spread.at[u, rng], x_out.at[c, si, rng], f_s.at[k, u], f_r.at[k, si], where)]
        if k == 0:
            out.append(remote(spreadt.at[u], rot_out.at[c, :, lanes(si)], f_s.at[PARTS, u], f_r.at[PARTS, si], where))
        return out

    def p_copy(ci, si, k):
        rng = pl.ds(k * half, half)
        out = [remote(x_out.at[ci, si, rng], x_out.at[ci, si, rng], p_s.at[k, si], p_r.at[k, si], here)]
        if k == 0:
            part = rot_out.at[ci, :, lanes(si)]
            out.append(remote(part, part, p_s.at[PARTS, si], p_r.at[PARTS, si], here))
        return out

    own_copies = [pltpu.make_async_copy(spread.at[s], x_out.at[c, s], own_s.at[0]),
                  pltpu.make_async_copy(spreadt.at[s], rot_out.at[c, :, lanes(s)], own_s.at[1])]

    def deliver(u, k):
        @pl.when(u != s)
        def _():
            each(f_copy(u, k, dev(u, z, c), s), "start")

        if k == PARTS - 1:
            @pl.when(u == s)
            def _():
                each(own_copies, "start")

    for k in range(PARTS):
        @pl.when(has_up)
        def _():
            each(g_copy(z, k, z + 1, 0), "start")

        @pl.when(has_down)
        def _():
            each(g_copy(z, k, z - 1, 1), "start")

        deliver(z, k)

    def g_step(d, carry):
        for k in range(PARTS):
            for sign in (-1, 1):
                u = z + sign * d

                @pl.when((u >= 0) & (u < planes))
                def _():
                    each(g_copy(u, k, z, 0), "wait_recv")
                    if sign < 0:
                        @pl.when(has_up)
                        def _():
                            each(g_copy(u, k, z + 1, 0), "start")
                    else:
                        @pl.when(has_down)
                        def _():
                            each(g_copy(u, k, z - 1, 1), "start")
                    deliver(u, k)
        return carry

    lax.fori_loop(1, planes, g_step, 0)
    each(own_copies, "wait")
    for k in range(PARTS):
        each(p_copy(c, s, k), "start")

    def p_step(i, carry):
        si = lax.rem(s + i, spots)
        for k in range(PARTS):
            each(f_copy(0, k, here, si), "wait_recv")
            each(p_copy(c, si, k), "start")
        return carry

    lax.fori_loop(1, spots, p_step, 0)

    def p_drain(si, carry):
        for k in range(PARTS):
            each(p_copy(1 - c, si, k), "wait_recv")
            each(p_copy(c, si, k), "wait_send")
        return carry

    lax.fori_loop(0, spots, p_drain, 0)

    def drain(u, carry):
        for k in range(PARTS):
            @pl.when(u != s)
            def _():
                each(f_copy(u, k, here, s), "wait_send")

            @pl.when((u <= z) & has_up)
            def _():
                each(g_copy(u, k, z, 0), "wait_send")

            @pl.when((u >= z) & has_down)
            def _():
                each(g_copy(u, k, z, 1), "wait_send")

        for k in range(3):
            @pl.when((u >= z) & has_down)
            def _():
                each(z_down(u, k), "wait_send")

            @pl.when((u < z) & has_up)
            def _():
                each(z_up(u, k), "wait_send")

        for k in range(2):
            @pl.when(u != z)
            def _():
                each(x_copy(u, k), "wait_send")
                each(y_copy(u, k), "wait_send")

        @pl.when((u != z) & by_y(u))
        def _():
            each(dy_copy(u), "wait_send")

        @pl.when((u != z) & ~by_y(u))
        def _():
            each(dx_copy(u), "wait_send")
        return carry

    lax.fori_loop(0, planes, drain, 0)

    @pl.when(has_up)
    def _():
        for k in range(3):
            each(z_own(k), "wait_send")


def read_kernel(x_ref, r_ref, up_ref, q_ref, cos_ref, sin_ref, plain_ref, value_ref, rot_ref, read_ref, wide):
    length = x_ref.shape[1]
    heads = q_ref.shape[1]
    lat = up_ref.shape[0]
    rope = r_ref.shape[1]
    kw = q_ref.shape[2] - rope
    vw = up_ref.shape[1] // heads - kw
    rotated = r_ref[0]
    rot_ref[0] = rotated
    normed = x_ref[0]
    keys = jnp.dot(normed, up_ref[:, :heads * kw], preferred_element_type=F32)
    values = jnp.dot(normed, up_ref[:, heads * kw:], preferred_element_type=F32)
    for h in range(heads):
        wide[pl.ds(h, length, stride=heads), :] = keys[:, h * kw:(h + 1) * kw]
    plain_ref[0] = wide[...].astype(BF16)
    for h in range(heads):
        wide[pl.ds(h, length, stride=heads), :] = values[:, h * vw:(h + 1) * vw]
    value_ref[0] = wide[...].astype(BF16)
    keys = keys.astype(BF16)
    values = values.astype(BF16)
    query = q_ref[0].astype(F32)
    turned = turn(query[:, kw:], cos_ref[...], sin_ref[...]).astype(BF16)
    tiled = jnp.concatenate([query[:, :kw]] * heads, axis=1)
    row = lax.broadcasted_iota(jnp.int32, tiled.shape, 0)
    col = lax.broadcasted_iota(jnp.int32, tiled.shape, 1)
    blocked = jnp.where(col // kw == row, tiled, 0.0).astype(BF16)
    contract = (((1,), (1,)), ((), ()))
    scores = lax.dot_general(blocked, keys, contract, preferred_element_type=F32)
    scores = scores + jnp.dot(turned, rotated, preferred_element_type=F32)
    scores = scores * (1.0 / (kw + rope) ** 0.5)
    weights = jnp.exp(scores - jnp.max(scores, axis=-1, keepdims=True))
    total = jnp.sum(weights, axis=-1, keepdims=True)
    mixed = jnp.dot(weights.astype(BF16), values, preferred_element_type=F32) / total
    for h in range(heads):
        read_ref[0, h:h + 1, :] = mixed[h:h + 1, h * vw:(h + 1) * vw].astype(BF16)


def body(planes, spots, tokens, latent_down, rope_weight, norm_scale, key_up, value_up, query):
    span = tokens.shape[1]
    rows, lat = latent_down.shape
    rope = rope_weight.shape[1]
    heads, kw = key_up.shape[1:]
    vw = value_up.shape[2]
    length = spots * span
    cosine, sine = turn_tables(np.arange(length + 1), rope)
    vmem = pl.BlockSpec(memory_space=pltpu.VMEM)
    hbm = pl.BlockSpec(memory_space=pl.ANY)
    dma = pltpu.SemaphoreType.DMA
    x_all, rot_all, up = pl.pallas_call(
        functools.partial(move_kernel, planes, spots),
        out_shape=(jax.ShapeDtypeStruct((CORES, spots, span, lat), BF16),
                   jax.ShapeDtypeStruct((CORES, rope, length), BF16),
                   jax.ShapeDtypeStruct((lat, heads * (kw + vw)), BF16)),
        in_specs=[hbm, hbm, hbm, vmem, hbm, hbm, hbm, hbm],
        out_specs=(vmem, vmem, vmem),
        scratch_shapes=[
            pltpu.VMEM((CORES, planes, span, rows), BF16),
            pltpu.VMEM((planes, rows, lat), BF16),
            pltpu.VMEM((planes, rope, rows), BF16),
            pltpu.VMEM((CORES * span, lat), F32),
            pltpu.VMEM((rope, CORES * span), F32),
            pltpu.VMEM((span, lat), F32),
            pltpu.VMEM((rope, span), F32),
            pltpu.VMEM((planes, span, lat), BF16),
            pltpu.VMEM((planes, rope, span), BF16),
            pltpu.VMEM(key_up.shape, BF16),
            pltpu.VMEM(value_up.shape, BF16),
            pltpu.VMEM((rope, span), F32),
            pltpu.VMEM((rope, span), F32),
            dma((planes,)), dma((planes,)), dma((planes + 2,)),
            dma((4, planes)), dma((4, planes)), dma((4,)),
            dma((3, planes)), dma((3, planes)), dma((3, planes)), dma((3, planes)),
            dma((3, planes)), dma((3, planes)), dma((3, planes)), dma((3, planes)),
            dma((2,)), dma((2,)),
            dma((2, PARTS + 1, planes)), dma((PARTS + 1, planes)),
            dma((PARTS + 1, planes)), dma((PARTS + 1, spots)),
            dma((PARTS + 1, spots)), dma((PARTS + 1, spots)),
            dma((4,)),
        ],
        compiler_params=pltpu.CompilerParams(collective_id=0, has_side_effects=True),
    )(tokens, latent_down, rope_weight.T, norm_scale.reshape(1, lat),
      jnp.asarray(np.ascontiguousarray(cosine[:length].T)), jnp.asarray(np.ascontiguousarray(sine[:length].T)),
      key_up, value_up)
    x_all = x_all.reshape(CORES, length, lat)

    def whole(shape):
        return pl.BlockSpec(shape, lambda i: (0,) * len(shape))

    def per(shape):
        return pl.BlockSpec((1,) + shape, lambda i: (i,) + (0,) * len(shape))

    plain, value, rot, read = pl.pallas_call(
        read_kernel,
        grid=(CORES,),
        out_shape=(jax.ShapeDtypeStruct((CORES, length * heads, kw), BF16),
                   jax.ShapeDtypeStruct((CORES, length * heads, vw), BF16),
                   jax.ShapeDtypeStruct((CORES, rope, length), BF16),
                   jax.ShapeDtypeStruct((CORES, heads, vw), BF16)),
        in_specs=[per((length, lat)), per((rope, length)), whole(up.shape), per(query.shape[1:]), whole((1, rope)), whole((1, rope))],
        out_specs=(per((length * heads, kw)), per((length * heads, vw)), per((rope, length)), per((heads, vw))),
        scratch_shapes=[pltpu.VMEM((length * heads, kw), F32)],
    )(x_all, rot_all, up, query, jnp.asarray(cosine[length:]), jnp.asarray(sine[length:]))
    return (plain.reshape(CORES, length, heads, kw), value.reshape(CORES, length, heads, vw), jnp.swapaxes(rot, 1, 2), read)


def solution(mesh):
    planes = mesh.shape["tp"] // CORES
    spots = mesh.shape["sp"]
    assert planes == spots and spots % 4 == 0
    in_specs = (
        P("tp", "sp", None),
        P("tp", None),
        P("tp", None),
        P(),
        P(None, "tp", None),
        P(None, "tp", None),
        P("sp", "tp", None),
    )
    out_specs = (
        P("sp", None, "tp", None),
        P("sp", None, "tp", None),
        P("sp", None, None),
        P("sp", "tp", None),
    )
    return jax.shard_map(functools.partial(body, planes, spots), mesh=mesh, in_specs=in_specs,
                         out_specs=out_specs, check_vma=False)
```

```python
import functools

import numpy as np
import jax
import jax.numpy as jnp
from jax import lax
from jax.sharding import PartitionSpec as P
from jax.experimental import pallas as pl
from jax.experimental.pallas import tpu as pltpu

CORES = 2
PARTS = 4
BF16 = jnp.bfloat16
F32 = jnp.float32


def turn_tables(positions, width):
    half = width // 2
    freqs = (1.0 / np.float32(10000.0) ** (np.arange(half, dtype=np.float32) * np.float32(2.0) / np.float32(width))).astype(np.float32)
    angles = positions.astype(np.float32)[:, None] * freqs
    cosine = np.cos(angles).astype(np.float32)
    sine = np.sin(angles).astype(np.float32)
    return np.concatenate([cosine, cosine], -1), np.concatenate([-sine, sine], -1)


def turn(part, cosine, sine):
    half = part.shape[-1] // 2
    swapped = jnp.concatenate([part[:, half:], part[:, :half]], axis=-1)
    return part * cosine + swapped * sine


def move_kernel(planes, spots, tok, wl, wr, scale, cos_hbm, sin_hbm, kup, vup, x_out, rot_out, up_out,
                tokens, wlat, wrope, acc, acct, other, othert, spread, spreadt, kbuf, vbuf, upbuf, cos_ref, sin_ref,
                tok_s, tok_r, own_s, z_s, z_r, zo_s, x_s, x_r, y_s, y_r, dx_s, dx_r, dy_s, dy_r,
                acc_s, acc_r, g_s, g_r, f_s, f_r, p_s, p_r, up_s):
    s = lax.axis_index("sp")
    t = lax.axis_index("tp")
    z = t // CORES
    c = t % CORES
    rows, lat = wl.shape
    rope = wr.shape[0]
    span = tok.shape[1]
    quarter = rows // 4
    eighth = quarter // 2
    rpart = rope // 4
    half = span // PARTS
    q = s % 4
    sx = s + 1 - 2 * (s % 2)
    sy = s + 2 - 4 * ((s // 2) % 2)
    qx = q + 1 - 2 * (q % 2)
    qy = q + 2 - 4 * (q // 2)
    qd = 3 - q

    def dev(si, zi, ci):
        return {"sp": si, "tp": zi * CORES + ci}

    here = dev(s, z, 1 - c)

    def remote(src, dst, ss, rs, where):
        return pltpu.make_async_remote_copy(
            src_ref=src, dst_ref=dst, send_sem=ss, recv_sem=rs,
            device_id=where, device_id_type=pl.DeviceIdType.MESH)

    def own_tok(u):
        cols = pl.ds(pl.multiple_of((u * CORES + c) * rows, 128), rows)
        return pltpu.make_async_copy(tok.at[0, :, cols], tokens.at[0, u], own_s.at[u])

    def part_tok(u):
        cols = pl.ds(pl.multiple_of((u * CORES + 1 - c) * rows, 128), rows)
        return remote(tok.at[0, :, cols], tokens.at[1, u], tok_s.at[u], tok_r.at[u], here)

    own_wl = pltpu.make_async_copy(wl, wlat.at[z], own_s.at[planes])
    own_wr = pltpu.make_async_copy(wr, wrope.at[z], own_s.at[planes + 1])
    place = pl.ds(pl.multiple_of(s * span, 128), span)
    get_k = pltpu.make_async_copy(kup, kbuf, up_s.at[0])
    get_v = pltpu.make_async_copy(vup, vbuf, up_s.at[1])
    get_c = pltpu.make_async_copy(cos_hbm.at[:, place], cos_ref, up_s.at[2])
    get_n = pltpu.make_async_copy(sin_hbm.at[:, place], sin_ref, up_s.at[3])
    own_wl.start()
    own_wr.start()

    barrier = pltpu.get_barrier_semaphore()

    def greet(where):
        pl.semaphore_signal(barrier, inc=1, device_id=where, device_id_type=pl.DeviceIdType.MESH)

    for i in range(1, planes):
        greet(dev(s, lax.rem(z + i, planes), c))
    for i in range(1, spots):
        greet(dev(lax.rem(s + i, spots), z, c))
    greet(here)
    for u in range(planes):
        own_tok(u).start()
    own_wl.wait()
    own_wr.wait()
    pl.semaphore_wait(barrier, planes - 1 + spots - 1 + 1)

    def piece(u, part, k, ss, rs, where):
        rng = pl.ds(pl.multiple_of(part * quarter + k * eighth, 16), eighth)
        out = [remote(wlat.at[u, rng], wlat.at[u, rng], ss.at[k, u], rs.at[k, u], where)]
        if k == 0:
            rng = pl.ds(pl.multiple_of(part * rpart, 16), rpart)
            out.append(remote(wrope.at[u, rng], wrope.at[u, rng], ss.at[2, u], rs.at[2, u], where))
        return out

    def each(copies, what):
        for p in copies:
            getattr(p, what)()

    def z_rows(k):
        start = q * quarter + k * eighth if k < 2 else qd * quarter + eighth
        return pl.ds(pl.multiple_of(start, 16), eighth)

    def z_piece(u, k, sems, where):
        rng = z_rows(k)
        i = k if k < 2 else 3
        out = [remote(wlat.at[u, rng], wlat.at[u, rng], sems(i), z_r.at[i, u], where)]
        if k == 0:
            rng = pl.ds(pl.multiple_of(q * rpart, 16), rpart)
            out.append(remote(wrope.at[u, rng], wrope.at[u, rng], sems(2), z_r.at[2, u], where))
        return out

    def z_own(k):
        return z_piece(z, k, lambda i: zo_s.at[i], dev(s, z + 1, c))

    def z_up(u, k):
        return z_piece(u, k, lambda i: z_s.at[i, u], dev(s, z + 1, c))

    def z_down(u, k):
        return z_piece(u, k, lambda i: z_s.at[i, u], dev(s, z - 1, c))

    def z_in(u, k):
        return z_piece(u, k, lambda i: z_s.at[i, u], here)

    def by_y(u):
        return (u + c) % 2 == 0

    def x_copy(u, k):
        return piece(u, q, k, x_s, x_r, dev(sx, z, c))

    def y_copy(u, k):
        return piece(u, q, k, y_s, y_r, dev(sy, z, c))

    def x_in(u, k):
        return piece(u, qx, k, x_s, x_r, here)

    def y_in(u, k):
        return piece(u, qy, k, y_s, y_r, here)

    def dy_copy(u):
        return piece(u, qx, 0, dy_s, dy_r, dev(sy, z, c))

    def dx_copy(u):
        return piece(u, qy, 0, dx_s, dx_r, dev(sx, z, c))

    def dy_in(u):
        return piece(u, qd, 0, dy_s, dy_r, here)

    def dx_in(u):
        return piece(u, qd, 0, dx_s, dx_r, here)

    has_up = z + 1 < planes
    has_down = z > 0
    for k in range(2):
        @pl.when(has_up)
        def _():
            each(z_own(k), "start")

        @pl.when(has_down)
        def _():
            each(z_down(z, k), "start")

    for u in range(planes):
        part_tok(u).start()
    get_k.start()
    get_v.start()
    get_c.start()
    get_n.start()
    contract = (((1,), (1,)), ((), ()))

    def block_dot(u):
        x = tokens[:, u].reshape(CORES * span, rows)
        return (jnp.dot(x, wlat[u], preferred_element_type=F32),
                lax.dot_general(wrope[u], x, contract, preferred_element_type=F32))

    def own_block():
        for u in range(planes):
            own_tok(u).wait()
            part_tok(u).wait()
        a, b = block_dot(z)
        acc[...] = a
        acct[...] = b

    put_up = pltpu.make_async_copy(upbuf, up_out, up_s.at[4])

    def reshape_up():
        get_k.wait()
        get_v.wait()
        get_c.wait()
        get_n.wait()
        heads, kw = kbuf.shape[1:]
        vw = vbuf.shape[2]
        k = kbuf[...].astype(F32)
        v = vbuf[...].astype(F32)
        for h in range(heads):
            upbuf[:, h * kw:(h + 1) * kw] = k[:, h, :].astype(BF16)
            upbuf[:, heads * kw + h * vw:heads * kw + (h + 1) * vw] = v[:, h, :].astype(BF16)
        put_up.start()

    def relay(u, k, sign):
        each(z_in(u, k), "wait_recv")
        if sign < 0:
            @pl.when(has_up)
            def _():
                each(z_up(u, k), "start")
        else:
            @pl.when(has_down)
            def _():
                each(z_down(u, k), "start")

    def send_own(k):
        @pl.when(has_up)
        def _():
            each(z_own(k), "start")

        @pl.when(has_down)
        def _():
            each(z_down(z, k), "start")

    def valid(u):
        return (u >= 0) & (u < planes)

    def step(d, carry):
        for k in range(2):
            for sign in (-1, 1):
                u = z + sign * d

                @pl.when(valid(u))
                def _():
                    relay(u, k, sign)
                    each(x_copy(u, k), "start")
                    each(y_copy(u, k), "start")

        @pl.when(d == 1)
        def _():
            own_block()

        @pl.when(d == 2)
        def _():
            reshape_up()

        @pl.when(d == planes - 1)
        def _():
            send_own(2)

        for sign in (-1, 1):
            u = z + sign * (d - 1)

            @pl.when(valid(u) & (d > 1))
            def _():
                @pl.when(by_y(u))
                def _():
                    each(x_in(u, 0), "wait_recv")
                    each(dy_copy(u), "start")

                @pl.when(~by_y(u))
                def _():
                    each(y_in(u, 0), "wait_recv")
                    each(dx_copy(u), "start")
        return carry

    lax.fori_loop(1, planes + 1, step, 0)

    def finish(d, carry):
        for sign in (-1, 1):
            u = z + sign * d

            @pl.when(valid(u))
            def _():
                relay(u, 2, sign)
        for sign in (-1, 1):
            u = z + sign * d

            @pl.when(valid(u))
            def _():
                each(x_in(u, 1), "wait_recv")
                each(y_in(u, 1), "wait_recv")

                @pl.when(by_y(u))
                def _():
                    each(y_in(u, 0), "wait_recv")
                    each(dy_in(u), "wait_recv")

                @pl.when(~by_y(u))
                def _():
                    each(x_in(u, 0), "wait_recv")
                    each(dx_in(u), "wait_recv")
                a, b = block_dot(u)
                acc[...] += a
                acct[...] += b
        return carry

    lax.fori_loop(1, planes, finish, 0)

    swaps = [remote(acc.at[pl.ds(span, span)], other, acc_s.at[0], acc_r.at[0], here),
             remote(acct.at[:, pl.ds(span, span)], othert, acc_s.at[1], acc_r.at[1], here)]
    each(swaps, "start")
    each(swaps, "wait")
    latent = acc[:span] + other[...]
    ropes = acct[:, :span] + othert[...]
    scaled = latent * lax.rsqrt(jnp.mean(latent * latent, axis=-1, keepdims=True) + 1e-06)
    spread[z] = (scaled * scale[...]).astype(BF16)
    swapped = jnp.concatenate([ropes[rope // 2:], ropes[:rope // 2]], axis=0)
    spreadt[z] = (ropes * cos_ref[...] + swapped * sin_ref[...]).astype(BF16)

    def g_copy(u, k, zi, slot):
        rng = pl.ds(k * half, half)
        out = [remote(spread.at[u, rng], spread.at[u, rng], g_s.at[slot, k, u], g_r.at[k, u], dev(s, zi, c))]
        if k == 0:
            out.append(remote(spreadt.at[u], spreadt.at[u], g_s.at[slot, PARTS, u], g_r.at[PARTS, u], dev(s, zi, c)))
        return out

    def lanes(si):
        return pl.ds(pl.multiple_of(si * span, 128), span)

    def f_copy(u, k, where, si):
        rng = pl.ds(k * half, half)
        out = [remote(spread.at[u, rng], x_out.at[c, si, rng], f_s.at[k, u], f_r.at[k, si], where)]
        if k == 0:
            out.append(remote(spreadt.at[u], rot_out.at[c, :, lanes(si)], f_s.at[PARTS, u], f_r.at[PARTS, si], where))
        return out

    def p_copy(ci, si, k):
        rng = pl.ds(k * half, half)
        out = [remote(x_out.at[ci, si, rng], x_out.at[ci, si, rng], p_s.at[k, si], p_r.at[k, si], here)]
        if k == 0:
            part = rot_out.at[ci, :, lanes(si)]
            out.append(remote(part, part, p_s.at[PARTS, si], p_r.at[PARTS, si], here))
        return out

    own_copies = [pltpu.make_async_copy(spread.at[s], x_out.at[c, s], own_s.at[0]),
                  pltpu.make_async_copy(spreadt.at[s], rot_out.at[c, :, lanes(s)], own_s.at[1])]

    def deliver(u, k):
        @pl.when(u != s)
        def _():
            each(f_copy(u, k, dev(u, z, c), s), "start")

        if k == PARTS - 1:
            @pl.when(u == s)
            def _():
                each(own_copies, "start")

    for k in range(PARTS):
        @pl.when(has_up)
        def _():
            each(g_copy(z, k, z + 1, 0), "start")

        @pl.when(has_down)
        def _():
            each(g_copy(z, k, z - 1, 1), "start")

        deliver(z, k)

    def g_step(d, carry):
        for k in range(PARTS):
            for sign in (-1, 1):
                u = z + sign * d

                @pl.when((u >= 0) & (u < planes))
                def _():
                    each(g_copy(u, k, z, 0), "wait_recv")
                    if sign < 0:
                        @pl.when(has_up)
                        def _():
                            each(g_copy(u, k, z + 1, 0), "start")
                    else:
                        @pl.when(has_down)
                        def _():
                            each(g_copy(u, k, z - 1, 1), "start")
                    deliver(u, k)
        return carry

    lax.fori_loop(1, planes, g_step, 0)
    each(own_copies, "wait")
    for k in range(PARTS):
        each(p_copy(c, s, k), "start")

    def p_step(i, carry):
        si = lax.rem(s + i, spots)
        for k in range(PARTS):
            each(f_copy(0, k, here, si), "wait_recv")
            each(p_copy(c, si, k), "start")
        return carry

    lax.fori_loop(1, spots, p_step, 0)

    def p_drain(si, carry):
        for k in range(PARTS):
            each(p_copy(1 - c, si, k), "wait_recv")
            each(p_copy(c, si, k), "wait_send")
        return carry

    lax.fori_loop(0, spots, p_drain, 0)

    def drain(u, carry):
        for k in range(PARTS):
            @pl.when(u != s)
            def _():
                each(f_copy(u, k, here, s), "wait_send")

            @pl.when((u <= z) & has_up)
            def _():
                each(g_copy(u, k, z, 0), "wait_send")

            @pl.when((u >= z) & has_down)
            def _():
                each(g_copy(u, k, z, 1), "wait_send")

        for k in range(3):
            @pl.when((u >= z) & has_down)
            def _():
                each(z_down(u, k), "wait_send")

            @pl.when((u < z) & has_up)
            def _():
                each(z_up(u, k), "wait_send")

        for k in range(2):
            @pl.when(u != z)
            def _():
                each(x_copy(u, k), "wait_send")
                each(y_copy(u, k), "wait_send")

        @pl.when((u != z) & by_y(u))
        def _():
            each(dy_copy(u), "wait_send")

        @pl.when((u != z) & ~by_y(u))
        def _():
            each(dx_copy(u), "wait_send")
        return carry

    lax.fori_loop(0, planes, drain, 0)
    put_up.wait()

    @pl.when(has_up)
    def _():
        for k in range(3):
            each(z_own(k), "wait_send")


def read_kernel(x_ref, r_ref, up_ref, q_ref, cos_ref, sin_ref, plain_ref, value_ref, rot_ref, read_ref, wide):
    length = x_ref.shape[1]
    heads = q_ref.shape[1]
    lat = up_ref.shape[0]
    rope = r_ref.shape[1]
    kw = q_ref.shape[2] - rope
    vw = up_ref.shape[1] // heads - kw
    rotated = r_ref[0]
    rot_ref[0] = rotated
    normed = x_ref[0]
    keys = jnp.dot(normed, up_ref[:, :heads * kw], preferred_element_type=F32)
    values = jnp.dot(normed, up_ref[:, heads * kw:], preferred_element_type=F32)
    for h in range(heads):
        wide[pl.ds(h, length, stride=heads), :] = keys[:, h * kw:(h + 1) * kw]
    plain_ref[0] = wide[...].astype(BF16)
    for h in range(heads):
        wide[pl.ds(h, length, stride=heads), :] = values[:, h * vw:(h + 1) * vw]
    value_ref[0] = wide[...].astype(BF16)
    keys = keys.astype(BF16)
    values = values.astype(BF16)
    query = q_ref[0].astype(F32)
    turned = turn(query[:, kw:], cos_ref[...], sin_ref[...]).astype(BF16)
    tiled = jnp.concatenate([query[:, :kw]] * heads, axis=1)
    row = lax.broadcasted_iota(jnp.int32, tiled.shape, 0)
    col = lax.broadcasted_iota(jnp.int32, tiled.shape, 1)
    blocked = jnp.where(col // kw == row, tiled, 0.0).astype(BF16)
    contract = (((1,), (1,)), ((), ()))
    scores = lax.dot_general(blocked, keys, contract, preferred_element_type=F32)
    scores = scores + jnp.dot(turned, rotated, preferred_element_type=F32)
    scores = scores * (1.0 / (kw + rope) ** 0.5)
    weights = jnp.exp(scores - jnp.max(scores, axis=-1, keepdims=True))
    total = jnp.sum(weights, axis=-1, keepdims=True)
    mixed = jnp.dot(weights.astype(BF16), values, preferred_element_type=F32) / total
    for h in range(heads):
        read_ref[0, h:h + 1, :] = mixed[h:h + 1, h * vw:(h + 1) * vw].astype(BF16)


def body(planes, spots, tokens, latent_down, rope_weight, norm_scale, key_up, value_up, query):
    span = tokens.shape[1]
    rows, lat = latent_down.shape
    rope = rope_weight.shape[1]
    heads, kw = key_up.shape[1:]
    vw = value_up.shape[2]
    length = spots * span
    cosine, sine = turn_tables(np.arange(length + 1), rope)
    vmem = pl.BlockSpec(memory_space=pltpu.VMEM)
    hbm = pl.BlockSpec(memory_space=pl.ANY)
    dma = pltpu.SemaphoreType.DMA
    x_all, rot_all, up = pl.pallas_call(
        functools.partial(move_kernel, planes, spots),
        out_shape=(jax.ShapeDtypeStruct((CORES, spots, span, lat), BF16),
                   jax.ShapeDtypeStruct((CORES, rope, length), BF16),
                   jax.ShapeDtypeStruct((lat, heads * (kw + vw)), BF16)),
        in_specs=[hbm, hbm, hbm, vmem, hbm, hbm, hbm, hbm],
        out_specs=(vmem, vmem, hbm),
        scratch_shapes=[
            pltpu.VMEM((CORES, planes, span, rows), BF16),
            pltpu.VMEM((planes, rows, lat), BF16),
            pltpu.VMEM((planes, rope, rows), BF16),
            pltpu.VMEM((CORES * span, lat), F32),
            pltpu.VMEM((rope, CORES * span), F32),
            pltpu.VMEM((span, lat), F32),
            pltpu.VMEM((rope, span), F32),
            pltpu.VMEM((planes, span, lat), BF16),
            pltpu.VMEM((planes, rope, span), BF16),
            pltpu.VMEM(key_up.shape, BF16),
            pltpu.VMEM(value_up.shape, BF16),
            pltpu.VMEM((lat, heads * (kw + vw)), BF16),
            pltpu.VMEM((rope, span), F32),
            pltpu.VMEM((rope, span), F32),
            dma((planes,)), dma((planes,)), dma((planes + 2,)),
            dma((4, planes)), dma((4, planes)), dma((4,)),
            dma((3, planes)), dma((3, planes)), dma((3, planes)), dma((3, planes)),
            dma((3, planes)), dma((3, planes)), dma((3, planes)), dma((3, planes)),
            dma((2,)), dma((2,)),
            dma((2, PARTS + 1, planes)), dma((PARTS + 1, planes)),
            dma((PARTS + 1, planes)), dma((PARTS + 1, spots)),
            dma((PARTS + 1, spots)), dma((PARTS + 1, spots)),
            dma((5,)),
        ],
        compiler_params=pltpu.CompilerParams(collective_id=0, has_side_effects=True),
    )(tokens, latent_down, rope_weight.T, norm_scale.reshape(1, lat),
      jnp.asarray(np.ascontiguousarray(cosine[:length].T)), jnp.asarray(np.ascontiguousarray(sine[:length].T)),
      key_up, value_up)
    x_all = x_all.reshape(CORES, length, lat)

    def whole(shape):
        return pl.BlockSpec(shape, lambda i: (0,) * len(shape))

    def per(shape):
        return pl.BlockSpec((1,) + shape, lambda i: (i,) + (0,) * len(shape))

    plain, value, rot, read = pl.pallas_call(
        read_kernel,
        grid=(CORES,),
        out_shape=(jax.ShapeDtypeStruct((CORES, length * heads, kw), BF16),
                   jax.ShapeDtypeStruct((CORES, length * heads, vw), BF16),
                   jax.ShapeDtypeStruct((CORES, rope, length), BF16),
                   jax.ShapeDtypeStruct((CORES, heads, vw), BF16)),
        in_specs=[per((length, lat)), per((rope, length)), whole(up.shape), per(query.shape[1:]), whole((1, rope)), whole((1, rope))],
        out_specs=(per((length * heads, kw)), per((length * heads, vw)), per((rope, length)), per((heads, vw))),
        scratch_shapes=[pltpu.VMEM((length * heads, kw), F32)],
    )(x_all, rot_all, up, query, jnp.asarray(cosine[length:]), jnp.asarray(sine[length:]))
    return (plain.reshape(CORES, length, heads, kw), value.reshape(CORES, length, heads, vw), jnp.swapaxes(rot, 1, 2), read)


def solution(mesh):
    planes = mesh.shape["tp"] // CORES
    spots = mesh.shape["sp"]
    assert planes == spots and spots % 4 == 0
    in_specs = (
        P("tp", "sp", None),
        P("tp", None),
        P("tp", None),
        P(),
        P(None, "tp", None),
        P(None, "tp", None),
        P("sp", "tp", None),
    )
    out_specs = (
        P("sp", None, "tp", None),
        P("sp", None, "tp", None),
        P("sp", None, None),
        P("sp", "tp", None),
    )
    return jax.shard_map(functools.partial(body, planes, spots), mesh=mesh, in_specs=in_specs,
                         out_specs=out_specs, check_vma=False)
```

```python
import functools

import numpy as np
import jax
import jax.numpy as jnp
from jax import lax
from jax.sharding import PartitionSpec as P
from jax.experimental import pallas as pl
from jax.experimental.pallas import tpu as pltpu

CORES = 2
PARTS = 4
BF16 = jnp.bfloat16
F32 = jnp.float32


def turn_tables(positions, width):
    half = width // 2
    freqs = (1.0 / np.float32(10000.0) ** (np.arange(half, dtype=np.float32) * np.float32(2.0) / np.float32(width))).astype(np.float32)
    angles = positions.astype(np.float32)[:, None] * freqs
    cosine = np.cos(angles).astype(np.float32)
    sine = np.sin(angles).astype(np.float32)
    return np.concatenate([cosine, cosine], -1), np.concatenate([-sine, sine], -1)


def turn(part, cosine, sine):
    half = part.shape[-1] // 2
    swapped = jnp.concatenate([part[:, half:], part[:, :half]], axis=-1)
    return part * cosine + swapped * sine


def move_kernel(planes, spots, tok, wl, wr, scale, cos_hbm, sin_hbm, kup, vup, x_out, rot_out, up_out,
                tokens, wlat, wrope, acc, acct, other, othert, spread, spreadt, kbuf, vbuf, upbuf, cos_ref, sin_ref,
                tok_s, tok_r, own_s, z_s, z_r, zo_s, x_s, x_r, y_s, y_r, dx_s, dx_r, dy_s, dy_r,
                acc_s, acc_r, g_s, g_r, f_s, f_r, p_s, p_r, up_s):
    s = lax.axis_index("sp")
    t = lax.axis_index("tp")
    z = t // CORES
    c = t % CORES
    rows, lat = wl.shape
    rope = wr.shape[0]
    span = tok.shape[1]
    quarter = rows // 4
    eighth = quarter // 2
    rpart = rope // 4
    half = span // PARTS
    q = s % 4
    sx = s + 1 - 2 * (s % 2)
    sy = s + 2 - 4 * ((s // 2) % 2)
    qx = q + 1 - 2 * (q % 2)
    qy = q + 2 - 4 * (q // 2)
    qd = 3 - q

    def dev(si, zi, ci):
        return {"sp": si, "tp": zi * CORES + ci}

    here = dev(s, z, 1 - c)

    def remote(src, dst, ss, rs, where):
        return pltpu.make_async_remote_copy(
            src_ref=src, dst_ref=dst, send_sem=ss, recv_sem=rs,
            device_id=where, device_id_type=pl.DeviceIdType.MESH)

    def own_tok(u):
        cols = pl.ds(pl.multiple_of((u * CORES + c) * rows, 128), rows)
        return pltpu.make_async_copy(tok.at[0, :, cols], tokens.at[0, u], own_s.at[u])

    def part_tok(u):
        cols = pl.ds(pl.multiple_of((u * CORES + 1 - c) * rows, 128), rows)
        return remote(tok.at[0, :, cols], tokens.at[1, u], tok_s.at[u], tok_r.at[u], here)

    own_wl = pltpu.make_async_copy(wl, wlat.at[z], own_s.at[planes])
    own_wr = pltpu.make_async_copy(wr, wrope.at[z], own_s.at[planes + 1])
    place = pl.ds(pl.multiple_of(s * span, 128), span)
    get_k = pltpu.make_async_copy(kup, kbuf, up_s.at[0])
    get_v = pltpu.make_async_copy(vup, vbuf, up_s.at[1])
    get_c = pltpu.make_async_copy(cos_hbm.at[:, place], cos_ref, up_s.at[2])
    get_n = pltpu.make_async_copy(sin_hbm.at[:, place], sin_ref, up_s.at[3])
    own_wl.start()
    own_wr.start()

    barrier = pltpu.get_barrier_semaphore()

    def greet(where):
        pl.semaphore_signal(barrier, inc=1, device_id=where, device_id_type=pl.DeviceIdType.MESH)

    for i in range(1, planes):
        greet(dev(s, lax.rem(z + i, planes), c))
    for i in range(1, spots):
        greet(dev(lax.rem(s + i, spots), z, c))
    greet(here)
    for u in range(planes):
        own_tok(u).start()
    own_wl.wait()
    own_wr.wait()
    pl.semaphore_wait(barrier, planes - 1 + spots - 1 + 1)

    def piece(u, part, k, ss, rs, where):
        rng = pl.ds(pl.multiple_of(part * quarter + k * eighth, 16), eighth)
        out = [remote(wlat.at[u, rng], wlat.at[u, rng], ss.at[k, u], rs.at[k, u], where)]
        if k == 0:
            rng = pl.ds(pl.multiple_of(part * rpart, 16), rpart)
            out.append(remote(wrope.at[u, rng], wrope.at[u, rng], ss.at[2, u], rs.at[2, u], where))
        return out

    def each(copies, what):
        for p in copies:
            getattr(p, what)()

    def z_rows(k):
        start = q * quarter + k * eighth if k < 2 else qd * quarter + eighth
        return pl.ds(pl.multiple_of(start, 16), eighth)

    def z_piece(u, k, sems, where):
        rng = z_rows(k)
        i = k if k < 2 else 3
        out = [remote(wlat.at[u, rng], wlat.at[u, rng], sems(i), z_r.at[i, u], where)]
        if k == 0:
            rng = pl.ds(pl.multiple_of(q * rpart, 16), rpart)
            out.append(remote(wrope.at[u, rng], wrope.at[u, rng], sems(2), z_r.at[2, u], where))
        return out

    def z_own(k):
        return z_piece(z, k, lambda i: zo_s.at[i], dev(s, z + 1, c))

    def z_up(u, k):
        return z_piece(u, k, lambda i: z_s.at[i, u], dev(s, z + 1, c))

    def z_down(u, k):
        return z_piece(u, k, lambda i: z_s.at[i, u], dev(s, z - 1, c))

    def z_in(u, k):
        return z_piece(u, k, lambda i: z_s.at[i, u], here)

    def by_y(u):
        return (u + c) % 2 == 0

    def x_copy(u, k):
        return piece(u, q, k, x_s, x_r, dev(sx, z, c))

    def y_copy(u, k):
        return piece(u, q, k, y_s, y_r, dev(sy, z, c))

    def x_in(u, k):
        return piece(u, qx, k, x_s, x_r, here)

    def y_in(u, k):
        return piece(u, qy, k, y_s, y_r, here)

    def dy_copy(u):
        return piece(u, qx, 0, dy_s, dy_r, dev(sy, z, c))

    def dx_copy(u):
        return piece(u, qy, 0, dx_s, dx_r, dev(sx, z, c))

    def dy_in(u):
        return piece(u, qd, 0, dy_s, dy_r, here)

    def dx_in(u):
        return piece(u, qd, 0, dx_s, dx_r, here)

    has_up = z + 1 < planes
    has_down = z > 0
    for k in range(2):
        @pl.when(has_up)
        def _():
            each(z_own(k), "start")

        @pl.when(has_down)
        def _():
            each(z_down(z, k), "start")

    for u in range(planes):
        part_tok(u).start()
    get_k.start()
    get_v.start()
    get_c.start()
    get_n.start()
    contract = (((1,), (1,)), ((), ()))

    def block_dot(u):
        x = tokens[:, u].reshape(CORES * span, rows)
        return (jnp.dot(x, wlat[u], preferred_element_type=F32),
                lax.dot_general(wrope[u], x, contract, preferred_element_type=F32))

    def own_block():
        for u in range(planes):
            own_tok(u).wait()
            part_tok(u).wait()
        a, b = block_dot(z)
        acc[...] = a
        acct[...] = b

    put_up = pltpu.make_async_copy(upbuf, up_out, up_s.at[4])

    def reshape_up():
        get_k.wait()
        get_v.wait()
        get_c.wait()
        get_n.wait()
        heads, kw = kbuf.shape[1:]
        vw = vbuf.shape[2]
        k = kbuf[...].astype(F32)
        v = vbuf[...].astype(F32)
        for h in range(heads):
            upbuf[:, h * kw:(h + 1) * kw] = k[:, h, :].astype(BF16)
            upbuf[:, heads * kw + h * vw:heads * kw + (h + 1) * vw] = v[:, h, :].astype(BF16)
        put_up.start()

    def relay(u, k, sign):
        each(z_in(u, k), "wait_recv")
        if sign < 0:
            @pl.when(has_up)
            def _():
                each(z_up(u, k), "start")
        else:
            @pl.when(has_down)
            def _():
                each(z_down(u, k), "start")

    def send_own(k):
        @pl.when(has_up)
        def _():
            each(z_own(k), "start")

        @pl.when(has_down)
        def _():
            each(z_down(z, k), "start")

    def valid(u):
        return (u >= 0) & (u < planes)

    def step(d, carry):
        for k in range(2):
            for sign in (-1, 1):
                u = z + sign * d

                @pl.when(valid(u))
                def _():
                    relay(u, k, sign)
                    each(x_copy(u, k), "start")
                    each(y_copy(u, k), "start")

        @pl.when(d == 1)
        def _():
            own_block()

        @pl.when(d == 2)
        def _():
            reshape_up()

        @pl.when(d == planes - 1)
        def _():
            send_own(2)

        for sign in (-1, 1):
            u = z + sign * (d - 1)

            @pl.when(valid(u) & (d > 1))
            def _():
                @pl.when(by_y(u))
                def _():
                    each(x_in(u, 0), "wait_recv")
                    each(dy_copy(u), "start")

                @pl.when(~by_y(u))
                def _():
                    each(y_in(u, 0), "wait_recv")
                    each(dx_copy(u), "start")
        return carry

    lax.fori_loop(1, planes + 1, step, 0)

    def finish(d, carry):
        for sign in (-1, 1):
            u = z + sign * d

            @pl.when(valid(u))
            def _():
                relay(u, 2, sign)
        for sign in (-1, 1):
            u = z + sign * d

            @pl.when(valid(u))
            def _():
                each(x_in(u, 1), "wait_recv")
                each(y_in(u, 1), "wait_recv")

                @pl.when(by_y(u))
                def _():
                    each(y_in(u, 0), "wait_recv")
                    each(dy_in(u), "wait_recv")

                @pl.when(~by_y(u))
                def _():
                    each(x_in(u, 0), "wait_recv")
                    each(dx_in(u), "wait_recv")
                a, b = block_dot(u)
                acc[...] += a
                acct[...] += b
        return carry

    lax.fori_loop(1, planes, finish, 0)

    swaps = [remote(acc.at[pl.ds(span, span)], other, acc_s.at[0], acc_r.at[0], here),
             remote(acct.at[:, pl.ds(span, span)], othert, acc_s.at[1], acc_r.at[1], here)]
    each(swaps, "start")
    each(swaps, "wait")
    latent = acc[:span] + other[...]
    ropes = acct[:, :span] + othert[...]
    scaled = latent * lax.rsqrt(jnp.mean(latent * latent, axis=-1, keepdims=True) + 1e-06)
    spread[z] = (scaled * scale[...]).astype(BF16)
    swapped = jnp.concatenate([ropes[rope // 2:], ropes[:rope // 2]], axis=0)
    spreadt[z] = (ropes * cos_ref[...] + swapped * sin_ref[...]).astype(BF16)

    def g_copy(u, k, zi, slot):
        rng = pl.ds(k * half, half)
        out = [remote(spread.at[u, rng], spread.at[u, rng], g_s.at[slot, k, u], g_r.at[k, u], dev(s, zi, c))]
        if k == 0:
            out.append(remote(spreadt.at[u], spreadt.at[u], g_s.at[slot, PARTS, u], g_r.at[PARTS, u], dev(s, zi, c)))
        return out

    def lanes(si):
        return pl.ds(pl.multiple_of(si * span, 128), span)

    def f_copy(u, k, where, si):
        rng = pl.ds(k * half, half)
        out = [remote(spread.at[u, rng], x_out.at[c, si, rng], f_s.at[k, u], f_r.at[k, si], where)]
        if k == 0:
            out.append(remote(spreadt.at[u], rot_out.at[c, :, lanes(si)], f_s.at[PARTS, u], f_r.at[PARTS, si], where))
        return out

    def p_copy(ci, si, k):
        rng = pl.ds(k * half, half)
        out = [remote(x_out.at[ci, si, rng], x_out.at[ci, si, rng], p_s.at[k, si], p_r.at[k, si], here)]
        if k == 0:
            part = rot_out.at[ci, :, lanes(si)]
            out.append(remote(part, part, p_s.at[PARTS, si], p_r.at[PARTS, si], here))
        return out

    own_copies = [pltpu.make_async_copy(spread.at[s], x_out.at[c, s], own_s.at[0]),
                  pltpu.make_async_copy(spreadt.at[s], rot_out.at[c, :, lanes(s)], own_s.at[1])]

    def deliver(u, k):
        @pl.when(u != s)
        def _():
            each(f_copy(u, k, dev(u, z, c), s), "start")

        if k == PARTS - 1:
            @pl.when(u == s)
            def _():
                each(own_copies, "start")

    for k in range(PARTS):
        @pl.when(has_up)
        def _():
            each(g_copy(z, k, z + 1, 0), "start")

        @pl.when(has_down)
        def _():
            each(g_copy(z, k, z - 1, 1), "start")

        deliver(z, k)

    def g_step(d, carry):
        for k in range(PARTS):
            for sign in (-1, 1):
                u = z + sign * d

                @pl.when((u >= 0) & (u < planes))
                def _():
                    each(g_copy(u, k, z, 0), "wait_recv")
                    if sign < 0:
                        @pl.when(has_up)
                        def _():
                            each(g_copy(u, k, z + 1, 0), "start")
                    else:
                        @pl.when(has_down)
                        def _():
                            each(g_copy(u, k, z - 1, 1), "start")
                    deliver(u, k)
        return carry

    lax.fori_loop(1, planes, g_step, 0)
    each(own_copies, "wait")
    for k in range(PARTS):
        each(p_copy(c, s, k), "start")

    for k in range(PARTS):
        def p_step(i, carry):
            si = lax.rem(s + i, spots)
            each(f_copy(0, k, here, si), "wait_recv")
            each(p_copy(c, si, k), "start")
            return carry

        lax.fori_loop(1, spots, p_step, 0)

    def p_drain(si, carry):
        for k in range(PARTS):
            each(p_copy(1 - c, si, k), "wait_recv")
            each(p_copy(c, si, k), "wait_send")
        return carry

    lax.fori_loop(0, spots, p_drain, 0)

    def drain(u, carry):
        for k in range(PARTS):
            @pl.when(u != s)
            def _():
                each(f_copy(u, k, here, s), "wait_send")

            @pl.when((u <= z) & has_up)
            def _():
                each(g_copy(u, k, z, 0), "wait_send")

            @pl.when((u >= z) & has_down)
            def _():
                each(g_copy(u, k, z, 1), "wait_send")

        for k in range(3):
            @pl.when((u >= z) & has_down)
            def _():
                each(z_down(u, k), "wait_send")

            @pl.when((u < z) & has_up)
            def _():
                each(z_up(u, k), "wait_send")

        for k in range(2):
            @pl.when(u != z)
            def _():
                each(x_copy(u, k), "wait_send")
                each(y_copy(u, k), "wait_send")

        @pl.when((u != z) & by_y(u))
        def _():
            each(dy_copy(u), "wait_send")

        @pl.when((u != z) & ~by_y(u))
        def _():
            each(dx_copy(u), "wait_send")
        return carry

    lax.fori_loop(0, planes, drain, 0)
    put_up.wait()

    @pl.when(has_up)
    def _():
        for k in range(3):
            each(z_own(k), "wait_send")


def read_kernel(x_ref, r_ref, up_ref, q_ref, cos_ref, sin_ref, plain_ref, value_ref, rot_ref, read_ref, wide):
    length = x_ref.shape[1]
    heads = q_ref.shape[1]
    lat = up_ref.shape[0]
    rope = r_ref.shape[1]
    kw = q_ref.shape[2] - rope
    vw = up_ref.shape[1] // heads - kw
    rotated = r_ref[0]
    rot_ref[0] = rotated
    normed = x_ref[0]
    keys = jnp.dot(normed, up_ref[:, :heads * kw], preferred_element_type=F32)
    values = jnp.dot(normed, up_ref[:, heads * kw:], preferred_element_type=F32)
    for h in range(heads):
        wide[pl.ds(h, length, stride=heads), :] = keys[:, h * kw:(h + 1) * kw]
    plain_ref[0] = wide[...].astype(BF16)
    for h in range(heads):
        wide[pl.ds(h, length, stride=heads), :] = values[:, h * vw:(h + 1) * vw]
    value_ref[0] = wide[...].astype(BF16)
    keys = keys.astype(BF16)
    values = values.astype(BF16)
    query = q_ref[0].astype(F32)
    turned = turn(query[:, kw:], cos_ref[...], sin_ref[...]).astype(BF16)
    tiled = jnp.concatenate([query[:, :kw]] * heads, axis=1)
    row = lax.broadcasted_iota(jnp.int32, tiled.shape, 0)
    col = lax.broadcasted_iota(jnp.int32, tiled.shape, 1)
    blocked = jnp.where(col // kw == row, tiled, 0.0).astype(BF16)
    contract = (((1,), (1,)), ((), ()))
    scores = lax.dot_general(blocked, keys, contract, preferred_element_type=F32)
    scores = scores + jnp.dot(turned, rotated, preferred_element_type=F32)
    scores = scores * (1.0 / (kw + rope) ** 0.5)
    weights = jnp.exp(scores - jnp.max(scores, axis=-1, keepdims=True))
    total = jnp.sum(weights, axis=-1, keepdims=True)
    mixed = jnp.dot(weights.astype(BF16), values, preferred_element_type=F32) / total
    for h in range(heads):
        read_ref[0, h:h + 1, :] = mixed[h:h + 1, h * vw:(h + 1) * vw].astype(BF16)


def body(planes, spots, tokens, latent_down, rope_weight, norm_scale, key_up, value_up, query):
    span = tokens.shape[1]
    rows, lat = latent_down.shape
    rope = rope_weight.shape[1]
    heads, kw = key_up.shape[1:]
    vw = value_up.shape[2]
    length = spots * span
    cosine, sine = turn_tables(np.arange(length + 1), rope)
    vmem = pl.BlockSpec(memory_space=pltpu.VMEM)
    hbm = pl.BlockSpec(memory_space=pl.ANY)
    dma = pltpu.SemaphoreType.DMA
    x_all, rot_all, up = pl.pallas_call(
        functools.partial(move_kernel, planes, spots),
        out_shape=(jax.ShapeDtypeStruct((CORES, spots, span, lat), BF16),
                   jax.ShapeDtypeStruct((CORES, rope, length), BF16),
                   jax.ShapeDtypeStruct((lat, heads * (kw + vw)), BF16)),
        in_specs=[hbm, hbm, hbm, vmem, hbm, hbm, hbm, hbm],
        out_specs=(vmem, vmem, hbm),
        scratch_shapes=[
            pltpu.VMEM((CORES, planes, span, rows), BF16),
            pltpu.VMEM((planes, rows, lat), BF16),
            pltpu.VMEM((planes, rope, rows), BF16),
            pltpu.VMEM((CORES * span, lat), F32),
            pltpu.VMEM((rope, CORES * span), F32),
            pltpu.VMEM((span, lat), F32),
            pltpu.VMEM((rope, span), F32),
            pltpu.VMEM((planes, span, lat), BF16),
            pltpu.VMEM((planes, rope, span), BF16),
            pltpu.VMEM(key_up.shape, BF16),
            pltpu.VMEM(value_up.shape, BF16),
            pltpu.VMEM((lat, heads * (kw + vw)), BF16),
            pltpu.VMEM((rope, span), F32),
            pltpu.VMEM((rope, span), F32),
            dma((planes,)), dma((planes,)), dma((planes + 2,)),
            dma((4, planes)), dma((4, planes)), dma((4,)),
            dma((3, planes)), dma((3, planes)), dma((3, planes)), dma((3, planes)),
            dma((3, planes)), dma((3, planes)), dma((3, planes)), dma((3, planes)),
            dma((2,)), dma((2,)),
            dma((2, PARTS + 1, planes)), dma((PARTS + 1, planes)),
            dma((PARTS + 1, planes)), dma((PARTS + 1, spots)),
            dma((PARTS + 1, spots)), dma((PARTS + 1, spots)),
            dma((5,)),
        ],
        compiler_params=pltpu.CompilerParams(collective_id=0, has_side_effects=True),
    )(tokens, latent_down, rope_weight.T, norm_scale.reshape(1, lat),
      jnp.asarray(np.ascontiguousarray(cosine[:length].T)), jnp.asarray(np.ascontiguousarray(sine[:length].T)),
      key_up, value_up)
    x_all = x_all.reshape(CORES, length, lat)

    def whole(shape):
        return pl.BlockSpec(shape, lambda i: (0,) * len(shape))

    def per(shape):
        return pl.BlockSpec((1,) + shape, lambda i: (i,) + (0,) * len(shape))

    plain, value, rot, read = pl.pallas_call(
        read_kernel,
        grid=(CORES,),
        out_shape=(jax.ShapeDtypeStruct((CORES, length * heads, kw), BF16),
                   jax.ShapeDtypeStruct((CORES, length * heads, vw), BF16),
                   jax.ShapeDtypeStruct((CORES, rope, length), BF16),
                   jax.ShapeDtypeStruct((CORES, heads, vw), BF16)),
        in_specs=[per((length, lat)), per((rope, length)), whole(up.shape), per(query.shape[1:]), whole((1, rope)), whole((1, rope))],
        out_specs=(per((length * heads, kw)), per((length * heads, vw)), per((rope, length)), per((heads, vw))),
        scratch_shapes=[pltpu.VMEM((length * heads, kw), F32)],
    )(x_all, rot_all, up, query, jnp.asarray(cosine[length:]), jnp.asarray(sine[length:]))
    return (plain.reshape(CORES, length, heads, kw), value.reshape(CORES, length, heads, vw), jnp.swapaxes(rot, 1, 2), read)


def solution(mesh):
    planes = mesh.shape["tp"] // CORES
    spots = mesh.shape["sp"]
    assert planes == spots and spots % 4 == 0
    in_specs = (
        P("tp", "sp", None),
        P("tp", None),
        P("tp", None),
        P(),
        P(None, "tp", None),
        P(None, "tp", None),
        P("sp", "tp", None),
    )
    out_specs = (
        P("sp", None, "tp", None),
        P("sp", None, "tp", None),
        P("sp", None, None),
        P("sp", "tp", None),
    )
    return jax.shard_map(functools.partial(body, planes, spots), mesh=mesh, in_specs=in_specs,
                         out_specs=out_specs, check_vma=False)
```
